512 devices in a mesh: sp: 64 (over z, y), tp: 8 (over x, core).
Axes of the slice: x: 4, y: 8, z: 8, core: 2. Of those that a mesh axis runs over, the one named last changes fastest.
Arguments:
- resid: bfloat16 [16384, 2048], P(('sp', 'tp')), may hold values from -6 to 6
- queries: bfloat16 [16384, 2048], P('sp', 'tp'), may hold values from -6 to 6
- keys: bfloat16 [16384, 1024], P('sp', 'tp'), may hold values from -6 to 6
- values: bfloat16 [16384, 1024], P('sp', 'tp'), may hold values from -6 to 6
- log_gates: float32 [16, 16384], P('tp'), as said below
- documents: int32 [16384], P('sp'), may hold values from 0 to 2, never falling along the last dimension, each value on 1 to 12288 neighbouring positions
- out_weight: bfloat16 [2048, 2048], P('tp'), may hold values from -0.125 to 0.125
- attn_gain: float32 [2048], replicated, may hold values from 0.1 to 1.9
- mlp_gain: float32 [2048], replicated, may hold values from 0.1 to 1.9
- gate_weight: bfloat16 [2048, 4096], P('sp', 'tp'), may hold values from -0.125 to 0.125
- up_weight: bfloat16 [2048, 4096], P('sp', 'tp'), may hold values from -0.125 to 0.125
- down_weight: bfloat16 [4096, 2048], P('tp', 'sp'), may hold values from -0.375 to 0.375
Outputs:
- mixed: bfloat16 [16384, 2048], P(('sp', 'tp'))
The draws below stay inside these ranges and needn't reach their ends.
Inputs may be any that keep to these rules, and one draw needn't show every extreme that they name: `log_gates`: each head's row never rises from one position to the next and starts at or below 0. `documents`: document numbers never fall along the positions; one document spans exactly three quarters of the 16384 positions.
All inputs are finite; a program needn't handle non-finite values.
Results may differ from the reference program's by a relative error of at most 0.018.
Values may be sent and summed in bfloat16 or wider, within the bound.
A program may use at most 64 MiB of HBM per device.

```python
import math
import jax
import jax.numpy as jnp
import numpy as np
from jax import lax

D = 2048
H = 16
KVH = 8
HD = 128
FF = 4096
TOKENS = 16384
ATT = 2048


def planted_pair(key):
    query_seed = jax.random.fold_in(key, 101)
    key_seed = jax.random.fold_in(key, 202)
    query_part = jnp.clip(jax.random.normal(query_seed, (TOKENS, H * HD), jnp.float32), -6.0, 6.0)
    key_part = jnp.clip(jax.random.normal(key_seed, (TOKENS, KVH * HD), jnp.float32), -6.0, 6.0)
    return (query_part, key_part)


def draw_queries(key, part):
    return planted_pair(key)[0].astype(jnp.bfloat16)


def draw_keys(key, part):
    return planted_pair(key)[1].astype(jnp.bfloat16)


def draw_log_gates(key, part):
    order_seed = jax.random.fold_in(key, 11)
    local_seed = jax.random.fold_in(key, 12)
    fast_seed = jax.random.fold_in(key, 13)
    slow_seed = jax.random.fold_in(key, 14)
    block_seed = jax.random.fold_in(key, 15)
    head_order = jax.random.permutation(order_seed, H)
    fast = head_order < H // 2
    local = jnp.exp(0.8 * jax.random.normal(local_seed, (H, TOKENS), jnp.float32))
    fast_rate = jnp.exp(jax.random.uniform(fast_seed, (H,), jnp.float32, math.log(1.0 / 150.0), math.log(1.0 / 45.0)))
    slow_rate = jnp.exp(jax.random.uniform(slow_seed, (H,), jnp.float32, math.log(0.3), math.log(1.2))) / TOKENS
    rate = jnp.where(fast, fast_rate, slow_rate)
    block_factor = jnp.exp(jax.random.uniform(block_seed, (H, TOKENS // 64), jnp.float32, math.log(0.5), math.log(2.0)))
    stretched = jnp.repeat(block_factor, 64, axis=1)
    return -jnp.cumsum(rate[:, None] * stretched * local, axis=1)


def block_levels(key, dims, split, smallest, top_value):
    level = 1.0
    for axis_at, blocks in split:
        steps = jax.random.uniform(jax.random.fold_in(jax.random.fold_in(key, 6), axis_at), (blocks,), jnp.float32, smallest / len(split), top_value / len(split))
        level = level * jnp.repeat(jnp.exp(steps), dims[axis_at] // blocks).reshape((-1,) + (1,) * (len(dims) - 1 - axis_at))
    return level


def length_profile(count, total, reach, lean):
    weights = [(1 << 20) // math.isqrt(standing ** lean) + 1 for standing in range(2, count + 1)]
    surplus, counts = total - reach - (count - 1), [1] * (count - 1)
    while surplus > 0:
        movable = [i for i in range(count - 1) if counts[i] < reach]
        mass, left = sum([weights[i] for i in movable]), surplus
        for i in movable:
            more = min(reach - counts[i], max(1, left * weights[i] // mass), surplus)
            counts[i] = counts[i] + more
            surplus = surplus - more
    return np.array([reach] + counts)


def ragged_sizes(own_key, count, total, limit, slope):
    if count == 2:
        one = jax.random.randint(own_key, (), max(1, total - limit), min(limit, total - 1) + 1)
        return jnp.stack([one, total - one])
    tallies = jnp.asarray(length_profile(count, total, limit, slope), jnp.int32)
    pairs = (count - 1) // 2
    giver, taker = tallies[1:1 + 2 * pairs:2], tallies[2:2 + 2 * pairs:2]
    slack = jnp.minimum(giver - 1, limit - taker)
    moved = jax.random.randint(jax.random.fold_in(own_key, 1), (pairs,), 0, 1 << 20) % (slack + 1)
    tallies = tallies.at[1:1 + 2 * pairs:2].set(giver - moved).at[2:2 + 2 * pairs:2].set(taker + moved)
    return tallies[jax.random.permutation(jax.random.fold_in(own_key, 2), count)]


def centred(rng, extent, spread, most, cuts=(), held_as=jnp.bfloat16):
    level = block_levels(rng, extent, cuts, -0.22, 0.18) if cuts else 1.0
    entries = jax.random.normal(rng, extent, jnp.float32) * spread * level
    return jnp.minimum(jnp.maximum(entries, -most), most).astype(held_as)


def setup_inputs(seed: int = 0) -> dict:
    splits = jax.random.split(jax.random.key(seed), 13)
    resid = centred(splits[0], (TOKENS, D), 1.0, 6.0, ((0, 512),))
    queries = draw_queries(jax.random.fold_in(splits[12], 71), 0)
    keys = draw_keys(jax.random.fold_in(splits[12], 71), 0)
    values = centred(splits[3], (TOKENS, KVH * HD), 1.0, 6.0, ((0, 64), (1, 8)))
    log_gates = draw_log_gates(jax.random.fold_in(splits[12], 71), 0)
    documents = jnp.searchsorted(jnp.cumsum(ragged_sizes(splits[5], 3, TOKENS, TOKENS * 3 // 4, 0)), jnp.arange(TOKENS), side="right").astype(jnp.int32)
    out_weight = centred(splits[6], (ATT, D), ATT ** -0.5, 0.125, ((0, 8),))
    attn_gain = jnp.clip(1.0 + 0.18 * jax.random.normal(splits[7], (D,), jnp.float32), 0.1, 1.9)
    mlp_gain = jnp.clip(1.0 + 0.18 * jax.random.normal(splits[8], (D,), jnp.float32), 0.1, 1.9)
    gate_weight = centred(splits[9], (D, FF), D ** -0.5, 0.125, ((0, 64), (1, 8)))
    up_weight = centred(splits[10], (D, FF), D ** -0.5, 0.125, ((0, 64), (1, 8)))
    down_weight = centred(splits[11], (FF, D), (FF // 16) ** -0.5, 0.375, ((0, 8), (1, 64)))
    return dict(resid=resid, queries=queries, keys=keys, values=values, log_gates=log_gates, documents=documents, out_weight=out_weight, attn_gain=attn_gain, mlp_gain=mlp_gain, gate_weight=gate_weight, up_weight=up_weight, down_weight=down_weight)


def reference(resid, queries, keys, values, log_gates, documents, out_weight, attn_gain, mlp_gain, gate_weight, up_weight, down_weight):
    group_size = H // KVH
    score_scale = 1.0 / math.sqrt(HD)
    key_heads = keys.reshape(TOKENS, KVH, HD).astype(jnp.float32)
    value_heads = values.reshape(TOKENS, KVH, HD).astype(jnp.float32)
    key_gates = log_gates.reshape(KVH, group_size, TOKENS)
    positions = jnp.arange(TOKENS, dtype=jnp.int32)
    block_len = math.gcd(TOKENS, 512)

    def attend(block_index):
        first_row = (block_index * block_len).astype(jnp.int32)
        query_block = lax.dynamic_slice_in_dim(queries, first_row, block_len, 0)
        query_block = query_block.reshape(block_len, KVH, group_size, HD).astype(jnp.float32)
        scores = jnp.einsum('tkgd,skd->kgts', query_block, key_heads) * score_scale
        query_gates = lax.dynamic_slice_in_dim(key_gates, first_row, block_len, 2)
        scores = scores + query_gates[..., None] - key_gates[:, :, None, :]
        query_pos = first_row + jnp.arange(block_len, dtype=jnp.int32)
        query_docs = lax.dynamic_slice_in_dim(documents, first_row, block_len, 0)
        visible = (positions[None, :] <= query_pos[:, None]) & (documents[None, :] == query_docs[:, None])
        scores = jnp.where(visible, scores, jnp.float32(-1e+30))
        row_max = lax.optimization_barrier(jnp.max(scores, axis=-1, keepdims=True))
        probs = jnp.where(visible, jnp.exp(scores - row_max), jnp.float32(0.0))
        row_sum = lax.optimization_barrier(jnp.sum(probs, axis=-1))
        probs_low = probs.astype(jnp.bfloat16).astype(jnp.float32)
        summed = jnp.einsum('kgts,skd->tkgd', probs_low, value_heads)
        summed = summed / jnp.transpose(row_sum, (2, 0, 1))[..., None]
        return summed.reshape(block_len, H * HD).astype(jnp.bfloat16)
    blocks = lax.map(attend, jnp.arange(TOKENS // block_len, dtype=jnp.int32))
    attended = blocks.reshape(TOKENS, H * HD)
    projected = jnp.dot(attended, out_weight, preferred_element_type=jnp.float32)
    power = lax.optimization_barrier(jnp.mean(projected * projected, axis=-1, keepdims=True))
    middle = resid.astype(jnp.float32) + attn_gain * projected * lax.rsqrt(power + 1e-06)
    middle_power = lax.optimization_barrier(jnp.mean(middle * middle, axis=-1, keepdims=True))
    normed = (mlp_gain * middle * lax.rsqrt(middle_power + 1e-06)).astype(jnp.bfloat16)
    gate_act = jnp.dot(normed, gate_weight, preferred_element_type=jnp.float32)
    up_act = jnp.dot(normed, up_weight, preferred_element_type=jnp.float32)
    hidden = (jax.nn.silu(gate_act) * up_act).astype(jnp.bfloat16)
    lowered = jnp.dot(hidden, down_weight, preferred_element_type=jnp.float32)
    return (middle + 0.5 * lowered).astype(jnp.bfloat16)
```

```python
import functools
import math

import jax
import jax.numpy as jnp
from jax import lax
from jax.experimental import pallas as pl
from jax.experimental.pallas import tpu as pltpu
from jax.sharding import PartitionSpec as P

HD = 128
MESH = pl.DeviceIdType.MESH
HIDE = -1e30
FLOOR = -1e20
AUG = 16
F32 = jnp.float32
BF16 = jnp.bfloat16
Y_DIM = 8
A_LANES = 128


def dot(a, b):
    return jnp.dot(a, b, preferred_element_type=F32)


class Ring:
    def __init__(self, n, pos, core, device, items, send_sem, recv_sem):
        self.n, self.pos, self.core, self.device, self.items = n, pos, core, device, items
        self.send_sem, self.recv_sem = send_sem, recv_sem
        self.last = n // 2 - 1
        self.copies = {}

    def at(self, step):
        return lax.rem(self.pos + step + 2 * self.n, self.n)

    def send(self, s, subs=None):
        for sub in range(len(self.items)) if subs is None else subs:
            if s < self.last:
                ways = [(0, self.at(-s), self.at(1)), (1, self.at(s), self.at(-1))]
            else:
                way = 1 - 2 * self.core
                ways = [(0, self.at(-way * s), self.at(way))]
            for d, item, to in ways:
                ref = self.items[sub](item)
                copy = pltpu.make_async_remote_copy(
                    src_ref=ref,
                    dst_ref=ref,
                    send_sem=self.send_sem.at[d, s, sub],
                    recv_sem=self.recv_sem.at[d, s, sub],
                    device_id=self.device(to),
                    device_id_type=MESH,
                )
                copy.start()
                self.copies[d, s, sub] = copy

    def wait(self, s, subs=None):
        for sub in range(len(self.items)) if subs is None else subs:
            for d in range(2 if s < self.last else 1):
                self.copies[d, s, sub].wait_recv()

    def arrived(self, s):
        if s < self.last:
            return [self.at(-1 - s), self.at(1 + s)]
        return [self.at(self.n // 2)]

    def finish(self):
        for copy in self.copies.values():
            copy.wait_send()


def layer_kernel(
    nz,
    ny,
    nx,
    back,
    resid,
    q,
    k,
    v,
    gates,
    docs,
    outw,
    attn_gain,
    mlp_gain,
    wpack,
    out,
    qa,
    kf,
    vt,
    osend,
    orecv,
    ssend,
    srecv,
    acc,
    att,
    asib,
    wsib,
    ps1,
    pr1,
    nrm,
    ps2,
    pr2,
    mid,
    wall,
    hid,
    low,
    q_ss,
    q_rs,
    k_ss,
    k_rs,
    a1_ss,
    a1_rs,
    b1_ss,
    b1_rs,
    a2_ss,
    a2_rs,
    b2_ss,
    b2_rs,
    fwd_ss,
    fwd_rs,
    o_ss,
    o_rs,
    t_ss,
    t_rs,
    x_ss,
    x_rs,
    c_ss,
    c_rs,
):
    sp, tp = lax.axis_index("sp"), lax.axis_index("tp")
    z, y = lax.div(sp, ny), lax.rem(sp, ny)
    x, c = lax.div(tp, 2), lax.rem(tp, 2)
    rows = q.shape[0]
    own_rows, width = resid.shape
    hidden = wpack.shape[2]
    scale = 1.0 / math.sqrt(HD)
    scale2 = scale * math.log2(math.e)
    la = A_LANES

    def along_z(i):
        return (i * ny + y, tp)

    def along_y(i):
        return (z * ny + i, tp)

    def along_x(i):
        return (sp, 2 * i + c)

    sibling = (sp, 2 * x + 1 - c)

    barrier = pltpu.get_barrier_semaphore()
    greet = [along_z(lax.rem(z + d, nz)) for d in ([1, nz - 1] if nz > 2 else [1])]
    greet += [along_y(lax.rem(y + d, ny)) for d in range(1, ny)]
    greet += [along_x(lax.rem(x + d, nx)) for d in range(1, nx)]
    greet += [sibling]
    for device in greet:
        pl.semaphore_signal(barrier, inc=1, device_id=device, device_id_type=MESH)

    row16 = lax.broadcasted_iota(jnp.int32, (AUG, rows), 0)
    doc16 = jnp.broadcast_to(docs[...], (AUG, rows))
    for h in range(2):
        qa[y, 0:HD, h * rows : (h + 1) * rows] = (
            q[:, h * HD : (h + 1) * HD].astype(F32).T.astype(BF16)
        )
        one_hot = jnp.where((row16 < 3) & (doc16 == row16), 1.0, 0.0)
        pick = jnp.where((row16 >= 3 + 3 * h) & (row16 < 6 + 3 * h), 1.0, 0.0)
        qa[y, HD : HD + AUG, h * rows : (h + 1) * rows] = (one_hot + pick).astype(BF16)
    kf[z, :, 0:HD] = k[...]
    vt[z, 0:HD, :] = v[...].astype(F32).T.astype(BF16)
    vt[z, HD : HD + AUG, :] = jnp.where(row16 == 0, doc16.astype(F32), 0.0).astype(BF16)

    pl.semaphore_wait(barrier, len(greet))

    def remote(src, dst, ss, rs, device):
        copy = pltpu.make_async_remote_copy(
            src_ref=src,
            dst_ref=dst,
            send_sem=ss,
            recv_sem=rs,
            device_id=device,
            device_id_type=MESH,
        )
        copy.start()
        return copy

    k_ring = Ring(
        nz,
        z,
        c,
        along_z,
        [lambda i: kf.at[i, :, 0:HD], lambda i: vt.at[i]],
        k_ss,
        k_rs,
    )
    q_ring = Ring(
        ny,
        y,
        c,
        along_y,
        [
            lambda i: qa.at[i, 0 : HD + AUG, 0:rows],
            lambda i: qa.at[i, 0 : HD + AUG, rows : 2 * rows],
        ],
        q_ss,
        q_rs,
    )
    a1 = Ring(nz, z, c, along_z, [lambda i: wall.at[c, :, i, y, :, 0:la]], a1_ss, a1_rs)
    b1 = Ring(ny, y, c, along_y, [lambda i: wall.at[c, :, z, i, :, la:hidden]], b1_ss, b1_rs)
    a2 = Ring(
        ny,
        y,
        c,
        along_y,
        [lambda i, w=w: wall.at[c, w, :, i, :, 0:la] for w in range(3)],
        a2_ss,
        a2_rs,
    )
    b2 = Ring(
        nz,
        z,
        c,
        along_z,
        [lambda i, w=w: wall.at[c, w, i, :, :, la:hidden] for w in range(3)],
        b2_ss,
        b2_rs,
    )

    k_ring.send(0)
    q_ring.send(0)
    wall[c, :, z, y] = wpack[...]
    a1.send(0)
    b1.send(0)
    core_copies = [remote(outw, wsib, c_ss.at[0], c_rs.at[0], sibling)]

    def zero_rows(i, _):
        qa[i, HD + AUG :, :] = jnp.zeros((qa.shape[1] - HD - AUG, 2 * rows), BF16)
        return 0

    lax.fori_loop(0, ny, zero_rows, 0)

    def key_terms(i):
        first = pl.multiple_of(rows * (i * ny + y), rows)
        raised = gates[:, pl.ds(first, rows)] * (-1.0 / scale)
        high = raised.astype(BF16).astype(F32)
        middle = (raised - high).astype(BF16).astype(F32)
        lowest = raised - high - middle
        key_docs = vt[i, HD : HD + AUG, :].astype(F32)[0:1, :]
        terms = jnp.where(row16.astype(F32) == key_docs, 0.0, HIDE)
        terms = jnp.where(row16 < 3, terms, 0.0)
        for h in range(2):
            for j, piece in enumerate((high, middle, lowest)):
                terms = jnp.where(row16 == 3 + 3 * h + j, piece[h : h + 1, :], terms)
        tall = jnp.concatenate([terms, jnp.zeros((HD - AUG, rows), F32)], axis=0)
        kf[i, :, HD : 2 * HD] = tall.T.astype(BF16)

    key_terms(z)
    for s in range(1, max(nz, ny) // 2 + 1):
        for ring in (k_ring, q_ring, a1, b1):
            if s - 1 <= ring.last:
                ring.wait(s - 1)
            if s <= ring.last:
                ring.send(s)
        if s - 1 <= k_ring.last:
            for i in k_ring.arrived(s - 1):
                key_terms(i)

    forwards = []

    def forward_a(i):
        piece = wall.at[c, :, :, i, :, 0:la]
        at = len(forwards)
        forwards.append(remote(piece, piece, fwd_ss.at[at], fwd_rs.at[at], sibling))

    def forward_b(i):
        piece = wall.at[c, :, i, :, :, la:hidden]
        at = len(forwards)
        forwards.append(remote(piece, piece, fwd_ss.at[at], fwd_rs.at[at], sibling))

    b2.send(0)
    a2.send(0)
    forward_b(z)
    forward_a(y)

    pending_b = [(s, w) for s in range(b2.last + 1) for w in range(3)]
    pending_a = [(s, w) for s in range(a2.last + 1) for w in range(3)]

    def relay(ring, pending, forward, count):
        for _ in range(count):
            if not pending:
                return
            s, w = pending.pop(0)
            ring.wait(s, [w])
            if s < ring.last:
                ring.send(s + 1, [w])
            if w == 2:
                for i in ring.arrived(s):
                    forward(i)

    def attend(step, own):
        if own:
            yq = y
        else:
            odd = lax.rem(step, 2)
            half = lax.div(step + 1, 2)
            yq = lax.rem(y + ny // 2 + jnp.where(odd == 1, -half, half) + ny, ny)
        queries = qa[yq]
        raw = dot(kf[z], queries)
        key_at = lax.broadcasted_iota(jnp.int32, raw.shape, 0)
        col = lax.broadcasted_iota(jnp.int32, raw.shape, 1)
        query_at = jnp.where(col >= rows, col - rows, col)
        raw = jnp.where(query_at - key_at + rows * (yq - y) >= 0, raw, HIDE)
        top = jnp.maximum(jnp.max(raw, axis=0, keepdims=True) * scale2, FLOOR)
        probs = jnp.exp2(raw * scale2 - top)
        total = jnp.sum(probs, axis=0, keepdims=True)
        acc[...] = dot(vt[z, 0:HD, :], probs.astype(BF16))

        def more(i, state):
            top, total = state
            raw = dot(kf[i], queries)
            new = jnp.maximum(top, jnp.max(raw, axis=0, keepdims=True) * scale2)
            probs = jnp.exp2(raw * scale2 - new)
            shrink = jnp.exp2(top - new)
            total = total * shrink + jnp.sum(probs, axis=0, keepdims=True)
            acc[...] = acc[...] * shrink + dot(vt[i, 0:HD, :], probs.astype(BF16))
            return new, total

        top, total = lax.fori_loop(jnp.maximum(z - back, 0), z, more, (top, total))
        row8 = lax.broadcasted_iota(jnp.int32, (8, 2 * rows), 0)
        stats = jnp.where(row8 == 0, top, total)
        if own:
            orecv[y] = acc[...].astype(BF16)
            srecv[y] = stats
        else:
            osend[yq] = acc[...].astype(BF16)
            ssend[yq] = stats
            remote(osend.at[yq], orecv.at[y], o_ss.at[step], o_rs.at[step], along_y(yq))
            remote(ssend.at[yq], srecv.at[y], t_ss.at[step], t_rs.at[step], along_y(yq))

    def attend_steps(first, past):
        if past > first:
            lax.fori_loop(first, past, lambda s, _: (attend(s, False), 0)[1], 0)

    cuts = [0, min(3, ny - 1), min(5, ny - 1), ny - 1]
    attend_steps(cuts[0], cuts[1])
    relay(b2, pending_b, forward_b, 1)
    attend_steps(cuts[1], cuts[2])
    relay(b2, pending_b, forward_b, 1)
    relay(a2, pending_a, forward_a, 2)
    attend_steps(cuts[2], cuts[3])
    relay(b2, pending_b, forward_b, 1)
    relay(a2, pending_a, forward_a, 1)
    attend(ny - 1, True)
    relay(b2, pending_b, forward_b, 2)

    for step in range(ny - 1):
        pltpu.make_async_remote_copy(
            src_ref=osend.at[0],
            dst_ref=orecv.at[0],
            send_sem=o_ss.at[step],
            recv_sem=o_rs.at[step],
            device_id=sibling,
            device_id_type=MESH,
        ).wait()
        pltpu.make_async_remote_copy(
            src_ref=ssend.at[0],
            dst_ref=srecv.at[0],
            send_sem=t_ss.at[step],
            recv_sem=t_rs.at[step],
            device_id=sibling,
            device_id_type=MESH,
        ).wait()

    top = srecv[0, 0:1, :]
    for i in range(1, ny):
        top = jnp.maximum(top, srecv[i, 0:1, :])
    acc[...] = jnp.zeros(acc.shape, F32)

    def join(i, total):
        share = jnp.exp2(srecv[i, 0:1, :] - top)
        acc[...] += orecv[i].astype(F32) * share
        return total + share * srecv[i, 1:2, :]

    total = lax.fori_loop(0, ny, join, jnp.zeros(top.shape, F32))
    joined = acc[...] / total
    for h in range(2):
        part = joined[:, h * rows : (h + 1) * rows].T.astype(BF16)
        att[:, :, :, h * HD : (h + 1) * HD] = part.reshape(nx, 2, own_rows, HD)
    core_copies.append(remote(att.at[:, 1 - c], asib, c_ss.at[1], c_rs.at[1], sibling))
    relay(b2, pending_b, forward_b, 1)
    relay(a2, pending_a, forward_a, 3)
    for copy in core_copies:
        copy.wait()

    core_rows = nx * own_rows
    mine = att[:, c].reshape(core_rows, 2 * HD)
    theirs = asib[...].reshape(core_rows, 2 * HD)
    chunk = min(512, width)
    for at in range(0, width, chunk):
        part = dot(mine, outw[:, at : at + chunk]) + dot(theirs, wsib[:, at : at + chunk])
        ps1[:, :, at : at + chunk] = part.astype(BF16).reshape(nx, own_rows, chunk)

    def to_owners(send, recv, which):
        copies = []
        for d in range(1, nx):
            to = lax.rem(x + d, nx)
            sems = (x_ss.at[which, d - 1], x_rs.at[which, d - 1])
            copies.append(remote(send.at[to], recv.at[x], *sems, along_x(to)))
        return copies

    def summed(send, recv):
        sums = send[x].astype(F32)
        for d in range(1, nx):
            sums = sums + recv[lax.rem(x + d, nx)].astype(F32)
        return sums

    copies = to_owners(ps1, pr1, 0)
    relay(b2, pending_b, forward_b, 1)
    relay(a2, pending_a, forward_a, 1)
    for copy in copies:
        copy.wait()
    projected = summed(ps1, pr1)
    power = jnp.mean(projected * projected, axis=-1, keepdims=True)
    middle = resid[...].astype(F32) + attn_gain[...] * projected * lax.rsqrt(power + 1e-06)
    mid[...] = middle
    middle_power = jnp.mean(middle * middle, axis=-1, keepdims=True)
    nrm[x] = (mlp_gain[...] * middle * lax.rsqrt(middle_power + 1e-06)).astype(BF16)
    copies = []
    for d in range(1, nx):
        sems = (x_ss.at[1, d - 1], x_rs.at[1, d - 1])
        copies.append(remote(nrm.at[x], nrm.at[x], *sems, along_x(lax.rem(x + d, nx))))
    relay(b2, pending_b, forward_b, 2)
    relay(a2, pending_a, forward_a, 2)
    for copy in copies:
        copy.wait()
    relay(b2, pending_b, forward_b, len(pending_b))
    relay(a2, pending_a, forward_a, len(pending_a))
    for copy in forwards:
        copy.wait()

    normed = nrm[...].reshape(core_rows, width)
    low[...] = jnp.zeros(low.shape, F32)

    def feed(j, _):
        gate = dot(normed, wall[j, 0].reshape(width, hidden))
        up = dot(normed, wall[j, 1].reshape(width, hidden))
        hid[...] = (gate / (1.0 + jnp.exp(-gate)) * up).astype(BF16)
        zs = max(1, chunk * nz // width)
        for at in range(0, nz, zs):
            w = wall[j, 2, at : at + zs].reshape(zs * width // nz, hidden)
            cols = slice(at * width // nz, (at + zs) * width // nz)
            low[:, cols] += lax.dot_general(
                hid[...], w, (((1,), (1,)), ((), ())), preferred_element_type=F32
            )
        return 0

    lax.fori_loop(0, 2, feed, 0)
    ps2[...] = low[...].astype(BF16).reshape(nx, own_rows, width)
    for copy in to_owners(ps2, pr2, 2):
        copy.wait()
    out[...] = (mid[...] + 0.5 * summed(ps2, pr2)).astype(BF16)
    for ring in (k_ring, q_ring, a1, b1, a2, b2):
        ring.finish()


def make_local(nz, ny, nx, back):
    def local(
        resid,
        queries,
        keys,
        values,
        log_gates,
        documents,
        out_weight,
        attn_gain,
        mlp_gain,
        gate_weight,
        up_weight,
        down_weight,
    ):
        rows = queries.shape[0]
        own_rows, width = resid.shape
        w_rows, hidden = gate_weight.shape
        wpack = jnp.stack([gate_weight, up_weight, down_weight.T])
        dma = pltpu.SemaphoreType.DMA
        x_block = pltpu.VMEM((nx, own_rows, width), BF16)
        kz, ky = nz // 2, ny // 2
        scratch = [
            pltpu.VMEM((ny, 2 * HD, 2 * rows), BF16),
            pltpu.VMEM((nz, rows, 2 * HD), BF16),
            pltpu.VMEM((nz, HD + AUG, rows), BF16),
            pltpu.VMEM((ny, HD, 2 * rows), BF16),
            pltpu.VMEM((ny, HD, 2 * rows), BF16),
            pltpu.VMEM((ny, 8, 2 * rows), F32),
            pltpu.VMEM((ny, 8, 2 * rows), F32),
            pltpu.VMEM((HD, 2 * rows), F32),
            pltpu.VMEM((nx, 2, own_rows, 2 * HD), BF16),
            pltpu.VMEM((nx, own_rows, 2 * HD), BF16),
            pltpu.VMEM(out_weight.shape, BF16),
            x_block,
            x_block,
            x_block,
            x_block,
            x_block,
            pltpu.VMEM((own_rows, width), F32),
            pltpu.VMEM((2, 3, nz, ny, w_rows, hidden), BF16),
            pltpu.VMEM((nx * own_rows, hidden), BF16),
            pltpu.VMEM((nx * own_rows, width), F32),
        ]
        for steps, subs in ((ky, 2), (kz, 2), (kz, 1), (ky, 1), (ky, 3), (kz, 3)):
            scratch += [dma((2, steps, subs)), dma((2, steps, subs))]
        scratch += [dma((nz + ny,)), dma((nz + ny,))]
        scratch += [dma((ny - 1,))] * 4
        scratch += [dma((3, max(nx - 1, 1)))] * 2
        scratch += [dma((2,)), dma((2,))]
        vmem = pl.BlockSpec(memory_space=pltpu.VMEM)
        return pl.pallas_call(
            functools.partial(layer_kernel, nz, ny, nx, back),
            out_shape=jax.ShapeDtypeStruct((own_rows, width), BF16),
            in_specs=[vmem] * 10,
            out_specs=vmem,
            scratch_shapes=scratch,
            compiler_params=pltpu.CompilerParams(
                collective_id=0, has_side_effects=True, vmem_limit_bytes=60 * 1024 * 1024
            ),
        )(
            resid,
            queries,
            keys,
            values,
            log_gates,
            documents.reshape(1, rows),
            out_weight,
            attn_gain.reshape(1, width),
            mlp_gain.reshape(1, width),
            wpack,
        )

    return local


def solution(mesh, ny=Y_DIM):
    blocks, tp = mesh.shape["sp"], mesh.shape["tp"]
    nz, nx = blocks // ny, tp // 2
    back = min((3 * blocks // 4 + ny - 1) // ny, nz - 1)
    placed = (
        P(("sp", "tp"), None),
        P("sp", "tp"),
        P("sp", "tp"),
        P("sp", "tp"),
        P("tp", None),
        P("sp"),
        P("tp", None),
        P(),
        P(),
        P("sp", "tp"),
        P("sp", "tp"),
        P("tp", "sp"),
    )
    return jax.shard_map(
        make_local(nz, ny, nx, back),
        mesh=mesh,
        in_specs=placed,
        out_specs=P(("sp", "tp"), None),
        check_vma=False,
    )
```

```python
import contextlib
import functools
import math

import jax
import jax.numpy as jnp
from jax import lax
from jax.experimental import pallas as pl
from jax.experimental.pallas import tpu as pltpu
from jax.sharding import PartitionSpec as P

HD = 128
MESH = pl.DeviceIdType.MESH
HIDE = -1e30
FLOOR = -1e20
AUG = 16
F32 = jnp.float32
BF16 = jnp.bfloat16
Y_DIM = 8
A_LANES = (128, 256, 256)
PROFILE = False


def phase(name):
    return jax.named_scope(name) if PROFILE else contextlib.nullcontext()


def dot(a, b):
    return jnp.dot(a, b, preferred_element_type=F32)


class Ring:
    def __init__(self, n, pos, core, device, items, send_sem, recv_sem):
        self.n, self.pos, self.core, self.device, self.items = n, pos, core, device, items
        self.send_sem, self.recv_sem = send_sem, recv_sem
        self.last = n // 2 - 1
        self.copies = {}

    def at(self, step):
        return lax.rem(self.pos + step + 2 * self.n, self.n)

    def send(self, s, subs=None):
        for sub in range(len(self.items)) if subs is None else subs:
            if s < self.last:
                ways = [(0, self.at(-s), self.at(1)), (1, self.at(s), self.at(-1))]
            else:
                way = 1 - 2 * self.core
                ways = [(0, self.at(-way * s), self.at(way))]
            for d, item, to in ways:
                ref = self.items[sub](item)
                copy = pltpu.make_async_remote_copy(
                    src_ref=ref,
                    dst_ref=ref,
                    send_sem=self.send_sem.at[d, s, sub],
                    recv_sem=self.recv_sem.at[d, s, sub],
                    device_id=self.device(to),
                    device_id_type=MESH,
                )
                copy.start()
                self.copies[d, s, sub] = copy

    def wait(self, s, subs=None):
        for sub in range(len(self.items)) if subs is None else subs:
            for d in range(2 if s < self.last else 1):
                self.copies[d, s, sub].wait_recv()

    def arrived(self, s):
        if s < self.last:
            return [self.at(-1 - s), self.at(1 + s)]
        return [self.at(self.n // 2)]

    def finish(self):
        for copy in self.copies.values():
            copy.wait_send()


def layer_kernel(
    nz,
    ny,
    nx,
    back,
    resid,
    q,
    k,
    v,
    gates,
    docs,
    outw,
    attn_gain,
    mlp_gain,
    wpack,
    out,
    qa,
    kf,
    vt,
    osend,
    oin,
    ssend,
    sin,
    stats,
    raw,
    acc,
    att,
    attall,
    wo,
    rall,
    nrm,
    ps2,
    pr2,
    mid,
    wall,
    gact,
    hid,
    low,
    q_ss,
    q_rs,
    k_ss,
    k_rs,
    a1_ss,
    a1_rs,
    b1_ss,
    b1_rs,
    a2_ss,
    a2_rs,
    b2_ss,
    b2_rs,
    fwd_ss,
    fwd_rs,
    o_ss,
    o_rs,
    t_ss,
    t_rs,
    x_ss,
    x_rs,
    w_ss,
    w_rs,
    wf_ss,
    wf_rs,
    g_ss,
    g_rs,
    l_ss,
):
    sp, tp = lax.axis_index("sp"), lax.axis_index("tp")
    z, y = lax.div(sp, ny), lax.rem(sp, ny)
    x, c = lax.div(tp, 2), lax.rem(tp, 2)
    rows = q.shape[0]
    own_rows, width = resid.shape
    hidden = wpack.shape[2]
    scale = 1.0 / math.sqrt(HD)
    scale2 = scale * math.log2(math.e)
    la = [min(lanes, hidden - 128) for lanes in A_LANES]

    def along_z(i):
        return (i * ny + y, tp)

    def along_y(i):
        return (z * ny + i, tp)

    def along_x(i):
        return (sp, 2 * i + c)

    sibling = (sp, 2 * x + 1 - c)

    barrier = pltpu.get_barrier_semaphore()
    greet = [along_z(lax.rem(z + d, nz)) for d in ([1, nz - 1] if nz > 2 else [1])]
    greet += [along_y(lax.rem(y + d, ny)) for d in range(1, ny)]
    greet += [along_x(lax.rem(x + d, nx)) for d in range(1, nx)]
    greet += [sibling]
    for device in greet:
        pl.semaphore_signal(barrier, inc=1, device_id=device, device_id_type=MESH)

    own_wo = pltpu.make_async_copy(outw, wo.at[tp], l_ss)
    own_wo.start()

    with phase("prep"):
        row16 = lax.broadcasted_iota(jnp.int32, (AUG, rows), 0)
        doc16 = jnp.broadcast_to(docs[...], (AUG, rows))
        for h in range(2):
            qa[y, 0:HD, h * rows : (h + 1) * rows] = (
                q[:, h * HD : (h + 1) * HD].astype(F32).T.astype(BF16)
            )
            one_hot = jnp.where((row16 < 3) & (doc16 == row16), 1.0, 0.0)
            pick = jnp.where((row16 >= 3 + 3 * h) & (row16 < 6 + 3 * h), 1.0, 0.0)
            qa[y, HD : HD + AUG, h * rows : (h + 1) * rows] = (one_hot + pick).astype(BF16)
        kf[z, :, 0:HD] = k[...]
        vt[z, 0:HD, :] = v[...].astype(F32).T.astype(BF16)
        vt[z, HD : HD + AUG, :] = jnp.where(row16 == 0, doc16.astype(F32), 0.0).astype(BF16)

    with phase("barrier_wait"):
        pl.semaphore_wait(barrier, len(greet))

    def remote(src, dst, ss, rs, device):
        copy = pltpu.make_async_remote_copy(
            src_ref=src,
            dst_ref=dst,
            send_sem=ss,
            recv_sem=rs,
            device_id=device,
            device_id_type=MESH,
        )
        copy.start()
        return copy

    k_ring = Ring(
        nz,
        z,
        c,
        along_z,
        [lambda i: kf.at[i, :, 0:HD], lambda i: vt.at[i]],
        k_ss,
        k_rs,
    )
    q_ring = Ring(
        ny,
        y,
        c,
        along_y,
        [
            lambda i: qa.at[i, 0 : HD + AUG, 0:rows],
            lambda i: qa.at[i, 0 : HD + AUG, rows : 2 * rows],
        ],
        q_ss,
        q_rs,
    )
    a1 = Ring(
        nz,
        z,
        c,
        along_z,
        [lambda i, w=w: wall.at[c, w, i, y, :, 0 : la[w]] for w in range(3)],
        a1_ss,
        a1_rs,
    )
    b1 = Ring(
        ny,
        y,
        c,
        along_y,
        [lambda i, w=w: wall.at[c, w, z, i, :, la[w] : hidden] for w in range(3)],
        b1_ss,
        b1_rs,
    )
    a2 = Ring(
        ny,
        y,
        c,
        along_y,
        [lambda i, w=w: wall.at[c, w, :, i, :, 0 : la[w]] for w in range(3)],
        a2_ss,
        a2_rs,
    )
    b2 = Ring(
        nz,
        z,
        c,
        along_z,
        [lambda i, w=w: wall.at[c, w, i, :, :, la[w] : hidden] for w in range(3)],
        b2_ss,
        b2_rs,
    )
    heads_half = outw.shape[0] // 2
    wo_ring = Ring(
        nx,
        x,
        c,
        along_x,
        [lambda i, u=u: wo.at[2 * i + c, u * heads_half : (u + 1) * heads_half] for u in range(2)],
        w_ss,
        w_rs,
    )

    wall[c, :, z, y] = wpack[...]
    k_ring.send(0, [0])
    q_ring.send(0, [0])
    a1.send(0)
    b1.send(0)
    k_ring.send(0, [1])
    q_ring.send(0, [1])

    wo_forwards = []

    def forward_wo(i, u):
        piece = wo.at[2 * i + c, u * heads_half : (u + 1) * heads_half]
        at = len(wo_forwards)
        wo_forwards.append(remote(piece, piece, wf_ss.at[at], wf_rs.at[at], sibling))

    own_wo.wait()
    if nx > 1:
        wo_ring.send(0)
    for u in range(2):
        forward_wo(x, u)
    pending_wo = [(s, u) for s in range(nx // 2) for u in range(2)]

    def relay_wo(count):
        for _ in range(min(count, len(pending_wo))):
            s, u = pending_wo.pop(0)
            with phase("wo_wait"):
                wo_ring.wait(s, [u])
            if s < wo_ring.last:
                wo_ring.send(s + 1, [u])
            for i in wo_ring.arrived(s):
                forward_wo(i, u)

    def zero_rows(i, _):
        qa[i, HD + AUG :, :] = jnp.zeros((qa.shape[1] - HD - AUG, 2 * rows), BF16)
        return 0

    lax.fori_loop(0, ny, zero_rows, 0)

    def key_terms(i):
        first = pl.multiple_of(rows * (i * ny + y), rows)
        raised = gates[:, pl.ds(first, rows)] * (-1.0 / scale)
        high = raised.astype(BF16).astype(F32)
        middle = (raised - high).astype(BF16).astype(F32)
        lowest = raised - high - middle
        key_docs = vt[i, HD : HD + AUG, :].astype(F32)[0:1, :]
        terms = jnp.where(row16.astype(F32) == key_docs, 0.0, HIDE)
        terms = jnp.where(row16 < 3, terms, 0.0)
        for h in range(2):
            for j, piece in enumerate((high, middle, lowest)):
                terms = jnp.where(row16 == 3 + 3 * h + j, piece[h : h + 1, :], terms)
        tall = jnp.concatenate([terms, jnp.zeros((HD - AUG, rows), F32)], axis=0)
        kf[i, :, HD : 2 * HD] = tall.T.astype(BF16)

    forwards = [[], [], []]

    def forward(piece, w):
        at = len(forwards[w])
        forwards[w].append(remote(piece, piece, fwd_ss.at[w, at], fwd_rs.at[w, at], sibling))

    def forward_a(i, w):
        forward(wall.at[c, w, :, i, :, 0 : la[w]], w)

    def forward_b(i, w):
        forward(wall.at[c, w, i, :, :, la[w] : hidden], w)

    def step_on(ring, s, subs):
        if s <= ring.last:
            for sub in subs:
                with phase("ring_wait"):
                    ring.wait(s, [sub])
                if s < ring.last:
                    ring.send(s + 1, [sub])

    key_terms(z)
    for s in range(max(nz, ny) // 2):
        step_on(k_ring, s, [0])
        step_on(q_ring, s, [0])
        step_on(a1, s, [0, 1, 2])
        step_on(b1, s, [0, 1, 2])
        if s == b1.last:
            b2.send(0)
        if s == a1.last:
            a2.send(0)
        step_on(k_ring, s, [1])
        step_on(q_ring, s, [1])
        if s <= k_ring.last:
            for i in k_ring.arrived(s):
                key_terms(i)
    for w in range(3):
        forward_b(z, w)
        forward_a(y, w)

    pending_b = [(s, w) for s in range(b2.last + 1) for w in range(3)]
    pending_a = [(s, w) for s in range(a2.last + 1) for w in range(3)]

    def relay(ring, pending, onward, count):
        for _ in range(min(count, len(pending))):
            s, w = pending.pop(0)
            with phase("relay_wait"):
                ring.wait(s, [w])
            if s < ring.last:
                ring.send(s + 1, [w])
            for i in ring.arrived(s):
                onward(i, w)

    def relay_a(count):
        relay(a2, pending_a, forward_a, count)

    def relay_b(count):
        relay(b2, pending_b, forward_b, count)

    half = ny // 2
    first_block = jnp.maximum(z - back, 0)
    count = z - first_block

    def query_block(step):
        odd = lax.rem(step, 2)
        turn = lax.div(step + 1, 2)
        return lax.rem(y + half + jnp.where(odd == 1, -turn, turn) + ny, ny)

    def fold(a, op):
        return op(a.reshape(rows // 8, 8, 2 * rows), axis=0)

    def score(slot, j, i, yq, diagonal):
        found = dot(kf[i], qa[yq])
        if diagonal:
            key_at = lax.broadcasted_iota(jnp.int32, found.shape, 0)
            col = lax.broadcasted_iota(jnp.int32, found.shape, 1)
            query_at = jnp.where(col >= rows, col - rows, col)
            found = jnp.where(query_at - key_at + rows * (yq - y) >= 0, found, HIDE)
        raw[slot, j] = found
        return fold(found, jnp.max)

    def weigh(slot, j, top):
        probs = jnp.exp2(raw[slot, j] * scale2 - top)
        return fold(probs, jnp.sum), probs.astype(BF16)

    def highest(top8):
        return jnp.maximum(jnp.max(top8, axis=0, keepdims=True) * scale2, FLOOR)

    def first_scores():
        yq = query_block(0)
        top8 = score(0, 0, z, yq, True)

        def more(j, top8):
            return jnp.maximum(top8, score(0, j, first_block + j - 1, yq, False))

        return lax.fori_loop(1, count + 1, more, top8)

    def attend(step, top8):
        slot = lax.rem(step, 2)
        top = highest(top8)
        ahead = query_block(step + 1)
        next8 = score(1 - slot, 0, z, ahead, True)
        sum8, probs = weigh(slot, 0, top)
        acc[...] = dot(vt[z, 0:HD, :], probs)

        def more(j, state):
            next8, sum8 = state
            i = first_block + j - 1
            next8 = jnp.maximum(next8, score(1 - slot, j, i, ahead, False))
            part8, probs = weigh(slot, j, top)
            acc[...] += dot(vt[i, 0:HD, :], probs)
            return next8, sum8 + part8

        next8, sum8 = lax.fori_loop(1, count + 1, more, (next8, sum8))
        row8 = lax.broadcasted_iota(jnp.int32, (8, 2 * rows), 0)
        stats[...] = jnp.where(row8 == 0, top, jnp.sum(sum8, axis=0, keepdims=True))
        return next8

    def lanes(h):
        return slice(h * rows, (h + 1) * rows)

    def out_copy(step, d, j, h, to):
        return pltpu.make_async_remote_copy(
            src_ref=osend.at[step, :, lanes(h)],
            dst_ref=oin.at[d, j, :, lanes(h)],
            send_sem=o_ss.at[step, h],
            recv_sem=o_rs.at[d, j, h],
            device_id=to,
            device_id_type=MESH,
        )

    def stat_copy(step, d, j, to):
        return pltpu.make_async_remote_copy(
            src_ref=ssend.at[step],
            dst_ref=sin.at[d, j],
            send_sem=t_ss.at[step],
            recv_sem=t_rs.at[d, j],
            device_id=to,
            device_id_type=MESH,
        )

    def add_arrived(d, j, after):
        with phase("o_wait"):
            stat_copy(0, d, j, sibling).wait_recv()
        top = stats[0:1, :]
        other = sin[d, j, 0:1, :]
        new = jnp.maximum(top, other)
        keep = jnp.exp2(top - new)
        take = jnp.exp2(other - new)
        total = stats[1:2, :] * keep + sin[d, j, 1:2, :] * take
        row8 = lax.broadcasted_iota(jnp.int32, (8, 2 * rows), 0)
        stats[...] = jnp.where(row8 == 0, new, total)
        for h in range(2):
            at = lanes(h)
            with phase("o_wait"):
                out_copy(0, d, j, h, sibling).wait_recv()
            acc[:, at] = acc[:, at] * keep[:, at] + oin[d, j, :, at].astype(F32) * take[:, at]
            after(h)

    def pass_on(step):
        j = half - (step + 1) // 2
        d = c if step == 0 else 1 - step % 2
        to = along_y(lax.rem(y + 1 - 2 * d + ny, ny))

        def send(h):
            if h == 0:
                ssend[step] = stats[...]
                stat_copy(step, d, j - 1, to).start()
            osend[step, :, lanes(h)] = acc[:, lanes(h)].astype(BF16)
            out_copy(step, d, j - 1, h, to).start()

        def plain():
            send(0)
            send(1)

        if step == 0:
            plain()
        elif j < half - 1:
            add_arrived(d, j, send)
        else:
            pl.when(c == d)(lambda: add_arrived(d, j, send))
            pl.when(c != d)(plain)

    with phase("first_scores"):
        top8 = first_scores()
    plan = {
        0: (0, 0, 1),
        1: (1, 1, 0),
        2: (1, 1, 0),
        3: (1, 1, 1),
        4: (0, 1, 0),
        5: (1, 1, 1),
        6: (1, 0, 0),
        7: (1, 1, 1),
    }
    for step in range(ny):
        with phase("attend"):
            top8 = attend(step, top8)
        if step < ny - 1:
            pass_on(step)
        count_b, count_a, count_wo = plan[step]
        relay_b(count_b)
        relay_a(count_a)
        relay_wo(count_wo)
    relay_wo(len(pending_wo))
    rall[x] = resid[...]
    copies_r = []
    for d in range(1, nx):
        sems = (x_ss.at[1, d - 1], x_rs.at[1, d - 1])
        copies_r.append(remote(rall.at[x], rall.at[x], *sems, along_x(lax.rem(x + d, nx))))
    for d in range(2):
        if half > 1:
            add_arrived(d, 0, lambda h: None)
        else:
            pl.when(c == d)(functools.partial(add_arrived, d, 0, lambda h: None))
    with phase("join"):
        joined = acc[...] / stats[1:2, :]
        for h in range(2):
            part = joined[:, lanes(h)].T.astype(BF16).reshape(nx, 2, own_rows, HD)
            for core in range(2):
                att[core, :, :, h * HD : (h + 1) * HD] = part[:, core]

    got = []
    for dx in range(nx):
        for dc in range(2):
            if dx + dc:
                to = (sp, 2 * lax.rem(x + dx, nx) + jnp.where(dc == 1, 1 - c, c))
                at = 2 * dx + dc - 1
                core = to[1] - 2 * lax.div(to[1], 2)
                copy = remote(att.at[core], attall.at[tp], g_ss.at[at], g_rs.at[at], to)
                source = 2 * lax.rem(x - dx + nx, nx) + jnp.where(dc == 1, 1 - c, c)
                got.append((copy, source, dx))
    core_rows = nx * own_rows
    chunk = min(512, width)
    relay_a(1)

    def project(first, block, source):
        for at in range(0, width, chunk):
            part = dot(block, wo[source, :, at : at + chunk])
            if first:
                low[:, at : at + chunk] = part
            else:
                low[:, at : at + chunk] += part

    with phase("outproj"):
        project(True, att[c].reshape(core_rows, 2 * HD), tp)
    with phase("fwo_wait"):
        for copy in wo_forwards:
            copy.wait()
    got.sort(key=lambda g: min(g[2], nx - g[2]))
    for n, (copy, source, _) in enumerate(got):
        with phase("ag_wait"):
            copy.wait()
        with phase("outproj"):
            project(False, attall[source].reshape(core_rows, 2 * HD), source)
        if n in (2, 4, 6):
            relay_b(1)
            relay_a(1 if n > 2 else 0)
    for copy in copies_r:
        copy.wait()

    def normalize(i, _):
        span = pl.ds(pl.multiple_of(i * own_rows, own_rows), own_rows)
        projected = low[span, :]
        power = jnp.mean(projected * projected, axis=-1, keepdims=True)
        middle = rall[i].astype(F32) + attn_gain[...] * projected * lax.rsqrt(power + 1e-06)
        mid[i] = middle
        middle_power = jnp.mean(middle * middle, axis=-1, keepdims=True)
        nrm[i] = (mlp_gain[...] * middle * lax.rsqrt(middle_power + 1e-06)).astype(BF16)
        return 0

    with phase("norm"):
        lax.fori_loop(0, nx, normalize, 0)
    while pending_b or pending_a:
        relay_b(1)
        relay_a(1)

    def forwarded(w):
        with phase("fwd_wait"):
            for copy in forwards[w]:
                copy.wait()

    normed = nrm[...].reshape(core_rows, width)

    def gate_core(j, _):
        gact[j] = dot(normed, wall[j, 0].reshape(width, hidden))
        return 0

    def up_core(j, _):
        gate = gact[j]
        up = dot(normed, wall[j, 1].reshape(width, hidden))
        hid[j] = (gate / (1.0 + jnp.exp(-gate)) * up).astype(BF16)
        return 0

    zs = max(1, chunk * nz // width)

    def down_cols(n, _):
        sums = 0.0
        for j in range(2):
            w = wall[j, 2, pl.ds(n * zs, zs)].reshape(zs * width // nz, hidden)
            sums += lax.dot_general(
                hid[j], w, (((1,), (1,)), ((), ())), preferred_element_type=F32
            )
        size = zs * width // nz
        cols = pl.ds(pl.multiple_of(n * size, size), size)
        ps2[:, :, cols] = sums.astype(BF16).reshape(nx, own_rows, size)
        return 0

    forwarded(0)
    with phase("ffn_gate"):
        lax.fori_loop(0, 2, gate_core, 0)
    forwarded(1)
    with phase("ffn_up"):
        lax.fori_loop(0, 2, up_core, 0)
    forwarded(2)
    with phase("ffn_down"):
        lax.fori_loop(0, nz // zs, down_cols, 0)

    def to_owners(send, recv, which):
        copies = []
        for d in range(1, nx):
            to = lax.rem(x + d, nx)
            sems = (x_ss.at[which, d - 1], x_rs.at[which, d - 1])
            copies.append(remote(send.at[to], recv.at[x], *sems, along_x(to)))
        return copies

    def summed(send, recv):
        sums = send[x].astype(F32)
        for d in range(1, nx):
            sums = sums + recv[lax.rem(x + d, nx)].astype(F32)
        return sums

    with phase("rs2_wait"):
        for copy in to_owners(ps2, pr2, 0):
            copy.wait()
    out[...] = (mid[x] + 0.5 * summed(ps2, pr2)).astype(BF16)
    for ring in (k_ring, q_ring, a1, b1, a2, b2, wo_ring):
        ring.finish()
    for step in range(ny - 1):
        stat_copy(step, 0, 0, sibling).wait_send()
        for h in range(2):
            out_copy(step, 0, 0, h, sibling).wait_send()


def make_local(nz, ny, nx, back):
    def local(
        resid,
        queries,
        keys,
        values,
        log_gates,
        documents,
        out_weight,
        attn_gain,
        mlp_gain,
        gate_weight,
        up_weight,
        down_weight,
    ):
        rows = queries.shape[0]
        own_rows, width = resid.shape
        w_rows, hidden = gate_weight.shape
        wpack = jnp.stack([gate_weight, up_weight, down_weight.T])
        dma = pltpu.SemaphoreType.DMA
        x_block = pltpu.VMEM((nx, own_rows, width), BF16)
        kz, ky = nz // 2, ny // 2
        scratch = [
            pltpu.VMEM((ny, 2 * HD, 2 * rows), BF16),
            pltpu.VMEM((nz, rows, 2 * HD), BF16),
            pltpu.VMEM((nz, HD + AUG, rows), BF16),
            pltpu.VMEM((ny - 1, HD, 2 * rows), BF16),
            pltpu.VMEM((2, ky, HD, 2 * rows), BF16),
            pltpu.VMEM((ny - 1, 8, 2 * rows), F32),
            pltpu.VMEM((2, ky, 8, 2 * rows), F32),
            pltpu.VMEM((8, 2 * rows), F32),
            pltpu.VMEM((2, back + 1, rows, 2 * rows), F32),
            pltpu.VMEM((HD, 2 * rows), F32),
            pltpu.VMEM((2, nx, own_rows, 2 * HD), BF16),
            pltpu.VMEM((2 * nx, nx, own_rows, 2 * HD), BF16),
            pltpu.VMEM((2 * nx, *out_weight.shape), BF16),
            x_block,
            x_block,
            x_block,
            x_block,
            pltpu.VMEM((nx, own_rows, width), F32),
            pltpu.VMEM((2, 3, nz, ny, w_rows, hidden), BF16),
            pltpu.VMEM((2, nx * own_rows, hidden), F32),
            pltpu.VMEM((2, nx * own_rows, hidden), BF16),
            pltpu.VMEM((nx * own_rows, width), F32),
        ]
        for steps, subs in ((ky, 2), (kz, 2), (kz, 3), (ky, 3), (ky, 3), (kz, 3)):
            scratch += [dma((2, steps, subs)), dma((2, steps, subs))]
        scratch += [dma((3, nz + ny)), dma((3, nz + ny))]
        scratch += [dma((ny - 1, 2)), dma((2, ky, 2)), dma((ny - 1,)), dma((2, ky))]
        scratch += [dma((2, max(nx - 1, 1)))] * 2
        scratch += [dma((2, max(nx // 2, 1), 2))] * 2
        scratch += [dma((2 * nx,))] * 2
        scratch += [dma((2 * nx,))] * 2
        scratch += [dma]
        vmem = pl.BlockSpec(memory_space=pltpu.VMEM)
        return pl.pallas_call(
            functools.partial(layer_kernel, nz, ny, nx, back),
            out_shape=jax.ShapeDtypeStruct((own_rows, width), BF16),
            in_specs=[vmem] * 6 + [pl.BlockSpec(memory_space=pl.ANY)] + [vmem] * 3,
            out_specs=vmem,
            scratch_shapes=scratch,
            compiler_params=pltpu.CompilerParams(
                collective_id=0, has_side_effects=True, vmem_limit_bytes=60 * 1024 * 1024
            ),
        )(
            resid,
            queries,
            keys,
            values,
            log_gates,
            documents.reshape(1, rows),
            out_weight,
            attn_gain.reshape(1, width),
            mlp_gain.reshape(1, width),
            wpack,
        )

    return local


def solution(mesh, ny=Y_DIM):
    blocks, tp = mesh.shape["sp"], mesh.shape["tp"]
    nz, nx = blocks // ny, tp // 2
    back = min((3 * blocks // 4 + ny - 1) // ny, nz - 1)
    placed = (
        P(("sp", "tp"), None),
        P("sp", "tp"),
        P("sp", "tp"),
        P("sp", "tp"),
        P("tp", None),
        P("sp"),
        P("tp", None),
        P(),
        P(),
        P("sp", "tp"),
        P("sp", "tp"),
        P("tp", "sp"),
    )
    return jax.shard_map(
        make_local(nz, ny, nx, back),
        mesh=mesh,
        in_specs=placed,
        out_specs=P(("sp", "tp"), None),
        check_vma=False,
    )
```

```python
import contextlib
import functools
import math

import jax
import jax.numpy as jnp
from jax import lax
from jax.experimental import pallas as pl
from jax.experimental.pallas import tpu as pltpu
from jax.sharding import PartitionSpec as P

HD = 128
MESH = pl.DeviceIdType.MESH
HIDE = -1e30
FLOOR = -1e20
AUG = 16
F32 = jnp.float32
BF16 = jnp.bfloat16
Y_DIM = 8
A_LANES = (128, 256, 256)
PROFILE = False


def phase(name):
    return jax.named_scope(name) if PROFILE else contextlib.nullcontext()


def dot(a, b):
    return jnp.dot(a, b, preferred_element_type=F32)


class Ring:
    def __init__(self, n, pos, core, device, items, send_sem, recv_sem):
        self.n, self.pos, self.core, self.device, self.items = n, pos, core, device, items
        self.send_sem, self.recv_sem = send_sem, recv_sem
        self.last = n // 2 - 1
        self.copies = {}

    def at(self, step):
        return lax.rem(self.pos + step + 2 * self.n, self.n)

    def send(self, s, subs=None):
        for sub in range(len(self.items)) if subs is None else subs:
            if s < self.last:
                ways = [(0, self.at(-s), self.at(1)), (1, self.at(s), self.at(-1))]
            else:
                way = 1 - 2 * self.core
                ways = [(0, self.at(-way * s), self.at(way))]
            for d, item, to in ways:
                ref = self.items[sub](item)
                copy = pltpu.make_async_remote_copy(
                    src_ref=ref,
                    dst_ref=ref,
                    send_sem=self.send_sem.at[d, s, sub],
                    recv_sem=self.recv_sem.at[d, s, sub],
                    device_id=self.device(to),
                    device_id_type=MESH,
                )
                copy.start()
                self.copies[d, s, sub] = copy

    def wait(self, s, subs=None):
        for sub in range(len(self.items)) if subs is None else subs:
            for d in range(2 if s < self.last else 1):
                self.copies[d, s, sub].wait_recv()

    def arrived(self, s):
        if s < self.last:
            return [self.at(-1 - s), self.at(1 + s)]
        return [self.at(self.n // 2)]

    def finish(self):
        for copy in self.copies.values():
            copy.wait_send()


def layer_kernel(
    nz,
    ny,
    nx,
    back,
    resid,
    q_in,
    k_in,
    v_in,
    gates_in,
    docs_in,
    outw,
    attn_gain_in,
    mlp_gain_in,
    gate_w,
    up_w,
    down_w,
    out,
    q,
    v,
    gates,
    docs,
    attn_gain,
    mlp_gain,
    qa,
    kf,
    vt,
    osend,
    oin,
    ssend,
    sin,
    stats,
    raw,
    acc,
    att,
    attall,
    wo,
    rall,
    nrm,
    ps2,
    pr2,
    mid,
    wall,
    gact,
    hid,
    low,
    q_ss,
    q_rs,
    k_ss,
    k_rs,
    a1_ss,
    a1_rs,
    b1_ss,
    b1_rs,
    a2_ss,
    a2_rs,
    b2_ss,
    b2_rs,
    fwd_ss,
    fwd_rs,
    o_ss,
    o_rs,
    t_ss,
    t_rs,
    x_ss,
    x_rs,
    w_ss,
    w_rs,
    wf_ss,
    wf_rs,
    g_ss,
    g_rs,
    s_ss,
    s_rs,
    l_ss,
):
    sp, tp = lax.axis_index("sp"), lax.axis_index("tp")
    z, y = lax.div(sp, ny), lax.rem(sp, ny)
    x, c = lax.div(tp, 2), lax.rem(tp, 2)
    rows = q.shape[0]
    own_rows, width = resid.shape
    hidden = gate_w.shape[1]
    scale = 1.0 / math.sqrt(HD)
    scale2 = scale * math.log2(math.e)
    la = [min(lanes, hidden - 128) for lanes in A_LANES]

    def along_z(i):
        return (i * ny + y, tp)

    def along_y(i):
        return (z * ny + i, tp)

    def along_x(i):
        return (sp, 2 * i + c)

    sibling = (sp, 2 * x + 1 - c)

    barrier = pltpu.get_barrier_semaphore()
    greet = [along_z(lax.rem(z + d, nz)) for d in ([1, nz - 1] if nz > 2 else [1])]
    greet += [along_y(lax.rem(y + d, ny)) for d in range(1, ny)]
    greet += [along_x(lax.rem(x + d, nx)) for d in range(1, nx)]
    greet += [sibling]
    for device in greet:
        pl.semaphore_signal(barrier, inc=1, device_id=device, device_id_type=MESH)

    loads = {}

    def load(name, src, dst):
        loads[name] = pltpu.make_async_copy(src, dst, l_ss.at[len(loads)])
        loads[name].start()

    load("q", q_in, q)
    load("docs", docs_in, docs)
    load("v", v_in, v)
    load("k", k_in, kf.at[z, :, 0:HD])
    load("gate", gate_w, wall.at[c, 0, z, y])
    load("up", up_w, wall.at[c, 1, z, y])
    load("down", down_w, wall.at[c, 2, z, y])
    load("gates", gates_in, gates)
    load("resid", resid, rall.at[x])
    load("wo", outw, wo.at[tp])
    load("attn_gain", attn_gain_in, attn_gain)
    load("mlp_gain", mlp_gain_in, mlp_gain)

    with phase("prep"):
        loads["docs"].wait()
        loads["q"].wait()
        row16 = lax.broadcasted_iota(jnp.int32, (AUG, rows), 0)
        doc16 = jnp.broadcast_to(docs[...], (AUG, rows))
        for h in range(2):
            qa[y, 0:HD, h * rows : (h + 1) * rows] = (
                q[:, h * HD : (h + 1) * HD].astype(F32).T.astype(BF16)
            )
            one_hot = jnp.where((row16 < 3) & (doc16 == row16), 1.0, 0.0)
            pick = jnp.where((row16 >= 3 + 3 * h) & (row16 < 6 + 3 * h), 1.0, 0.0)
            qa[y, HD : HD + AUG, h * rows : (h + 1) * rows] = (one_hot + pick).astype(BF16)
        loads["v"].wait()
        vt[z, 0:HD, :] = v[...].astype(F32).T.astype(BF16)
        vt[z, HD : HD + AUG, :] = jnp.where(row16 == 0, doc16.astype(F32), 0.0).astype(BF16)
        for name in ("k", "gate", "up", "down"):
            loads[name].wait()

    with phase("barrier_wait"):
        pl.semaphore_wait(barrier, len(greet))

    def remote(src, dst, ss, rs, device):
        copy = pltpu.make_async_remote_copy(
            src_ref=src,
            dst_ref=dst,
            send_sem=ss,
            recv_sem=rs,
            device_id=device,
            device_id_type=MESH,
        )
        copy.start()
        return copy

    k_ring = Ring(
        nz,
        z,
        c,
        along_z,
        [lambda i: kf.at[i, :, 0:HD], lambda i: vt.at[i]],
        k_ss,
        k_rs,
    )
    q_ring = Ring(
        ny,
        y,
        c,
        along_y,
        [
            lambda i: qa.at[i, 0 : HD + AUG, 0:rows],
            lambda i: qa.at[i, 0:HD, rows : 2 * rows],
        ],
        q_ss,
        q_rs,
    )
    a1 = Ring(
        nz,
        z,
        c,
        along_z,
        [lambda i, w=w: wall.at[c, w, i, y, :, 0 : la[w]] for w in range(3)],
        a1_ss,
        a1_rs,
    )
    b1 = Ring(
        ny,
        y,
        c,
        along_y,
        [lambda i, w=w: wall.at[c, w, z, i, :, la[w] : hidden] for w in range(3)],
        b1_ss,
        b1_rs,
    )
    a2 = Ring(
        ny,
        y,
        c,
        along_y,
        [lambda i, w=w: wall.at[c, w, :, i, :, 0 : la[w]] for w in range(3)],
        a2_ss,
        a2_rs,
    )
    b2 = Ring(
        nz,
        z,
        c,
        along_z,
        [lambda i, w=w: wall.at[c, w, i, :, :, la[w] : hidden] for w in range(3)],
        b2_ss,
        b2_rs,
    )
    heads_half = outw.shape[0] // 2
    wo_ring = Ring(
        nx,
        x,
        c,
        along_x,
        [lambda i, u=u: wo.at[2 * i + c, u * heads_half : (u + 1) * heads_half] for u in range(2)],
        w_ss,
        w_rs,
    )

    k_ring.send(0, [0])
    q_ring.send(0, [0])
    a1.send(0)
    b1.send(0)
    k_ring.send(0, [1])
    q_ring.send(0, [1])

    wo_forwards = []
    wo_at = {i: [] for i in range(nx)}

    def forward_wo(i, u, rel):
        piece = wo.at[2 * i + c, u * heads_half : (u + 1) * heads_half]
        at = len(wo_forwards)
        wo_at[rel % nx].append(at)
        wo_forwards.append(remote(piece, piece, wf_ss.at[at], wf_rs.at[at], sibling))

    loads["resid"].wait()
    copies_r = []
    for d in range(1, nx):
        sems = (x_ss.at[1, d - 1], x_rs.at[1, d - 1])
        copies_r.append(remote(rall.at[x], rall.at[x], *sems, along_x(lax.rem(x + d, nx))))
    loads["wo"].wait()
    if nx > 1:
        wo_ring.send(0)
    for u in range(2):
        forward_wo(x, u, 0)
    pending_wo = [(s, u) for s in range(nx // 2) for u in range(2)]

    def relay_wo(count):
        for _ in range(min(count, len(pending_wo))):
            s, u = pending_wo.pop(0)
            with phase("wo_wait"):
                wo_ring.wait(s, [u])
            if s < wo_ring.last:
                wo_ring.send(s + 1, [u])
            rels = (-1 - s, 1 + s) if s < wo_ring.last else (nx // 2,)
            for i, rel in zip(wo_ring.arrived(s), rels):
                forward_wo(i, u, rel)

    def second_head(i):
        seen = qa[i, HD : HD + AUG, 0:rows].astype(F32)
        pick = jnp.where((row16 >= 6) & (row16 < 9), 1.0, 0.0)
        qa[i, HD : HD + AUG, rows : 2 * rows] = jnp.where(row16 < 3, seen, pick).astype(BF16)

    def zero_rows(i, _):
        qa[i, HD + AUG :, :] = jnp.zeros((qa.shape[1] - HD - AUG, 2 * rows), BF16)
        return 0

    lax.fori_loop(0, ny, zero_rows, 0)

    def key_terms(i):
        first = pl.multiple_of(rows * (i * ny + y), rows)
        raised = gates[:, pl.ds(first, rows)] * (-1.0 / scale)
        high = raised.astype(BF16).astype(F32)
        middle = (raised - high).astype(BF16).astype(F32)
        lowest = raised - high - middle
        key_docs = vt[i, HD : HD + AUG, :].astype(F32)[0:1, :]
        terms = jnp.where(row16.astype(F32) == key_docs, 0.0, HIDE)
        terms = jnp.where(row16 < 3, terms, 0.0)
        for h in range(2):
            for j, piece in enumerate((high, middle, lowest)):
                terms = jnp.where(row16 == 3 + 3 * h + j, piece[h : h + 1, :], terms)
        tall = jnp.concatenate([terms, jnp.zeros((HD - AUG, rows), F32)], axis=0)
        kf[i, :, HD : 2 * HD] = tall.T.astype(BF16)

    forwards = [[], [], []]

    def forward(piece, w):
        at = len(forwards[w])
        forwards[w].append(remote(piece, piece, fwd_ss.at[w, at], fwd_rs.at[w, at], sibling))

    def forward_a(i, w):
        forward(wall.at[c, w, :, i, :, 0 : la[w]], w)

    def forward_b(i, w):
        forward(wall.at[c, w, i, :, :, la[w] : hidden], w)

    def step_on(ring, s, subs):
        if s <= ring.last:
            for sub in subs:
                with phase("ring_wait"):
                    ring.wait(s, [sub])
                if s < ring.last:
                    ring.send(s + 1, [sub])

    loads["gates"].wait()
    key_terms(z)
    for s in range(max(nz, ny) // 2):
        step_on(k_ring, s, [0])
        step_on(q_ring, s, [0])
        if s <= q_ring.last:
            for i in q_ring.arrived(s):
                second_head(i)
        step_on(a1, s, [0, 1, 2])
        step_on(b1, s, [0, 1, 2])
        if s == b1.last:
            b2.send(0)
        if s == a1.last:
            a2.send(0, [0, 1])
        step_on(k_ring, s, [1])
        step_on(q_ring, s, [1])
        if s <= k_ring.last:
            for i in k_ring.arrived(s):
                key_terms(i)
    for w in range(3):
        forward_b(z, w)
        if w < 2:
            forward_a(y, w)

    pending_b = [(s, w) for s in range(b2.last + 1) for w in range(3)]
    pending_a = [(s, w) for s in range(a2.last + 1) for w in range(2)]
    late_a = [(s, 2) for s in range(a2.last + 1)]

    def start_late():
        a2.send(0, [2])
        forward_a(y, 2)

    def relay_late():
        relay(a2, late_a, forward_a, 1)

    def relay(ring, pending, onward, count):
        for _ in range(min(count, len(pending))):
            s, w = pending.pop(0)
            with phase("relay_wait"):
                ring.wait(s, [w])
            if s < ring.last:
                ring.send(s + 1, [w])
            for i in ring.arrived(s):
                onward(i, w)

    def relay_a(count):
        relay(a2, pending_a, forward_a, count)

    def relay_b(count):
        relay(b2, pending_b, forward_b, count)

    half = ny // 2
    first_block = jnp.maximum(z - back, 0)
    count = z - first_block

    def query_block(step):
        d = 1 - c if step % 2 else c
        return lax.rem(y + (half - (step + 1) // 2) * (1 - 2 * d) + ny, ny)

    def fold(a, op):
        return op(a.reshape(rows // 8, 8, 2 * rows), axis=0)

    def score(slot, j, i, yq, diagonal):
        found = dot(kf[i], qa[yq])
        if diagonal:
            key_at = lax.broadcasted_iota(jnp.int32, found.shape, 0)
            col = lax.broadcasted_iota(jnp.int32, found.shape, 1)
            query_at = jnp.where(col >= rows, col - rows, col)
            found = jnp.where(query_at - key_at + rows * (yq - y) >= 0, found, HIDE)
        raw[slot, j] = found
        return fold(found, jnp.max)

    def weigh(slot, j, top):
        probs = jnp.exp2(raw[slot, j] * scale2 - top)
        return fold(probs, jnp.sum), probs.astype(BF16)

    def highest(top8):
        return jnp.maximum(jnp.max(top8, axis=0, keepdims=True) * scale2, FLOOR)

    def first_scores():
        yq = query_block(0)
        top8 = score(0, 0, z, yq, True)

        def more(j, top8):
            return jnp.maximum(top8, score(0, j, first_block + j - 1, yq, False))

        return lax.fori_loop(1, count + 1, more, top8)

    def attend(step, top8):
        slot = step % 2
        top = highest(top8)
        ahead = query_block(min(step + 1, ny - 1))
        next8 = score(1 - slot, 0, z, ahead, True)
        sum8, probs = weigh(slot, 0, top)
        acc[...] = dot(vt[z, 0:HD, :], probs)

        def more(j, state):
            next8, sum8 = state
            i = first_block + j - 1
            next8 = jnp.maximum(next8, score(1 - slot, j, i, ahead, False))
            part8, probs = weigh(slot, j, top)
            acc[...] += dot(vt[i, 0:HD, :], probs)
            return next8, sum8 + part8

        next8, sum8 = lax.fori_loop(1, count + 1, more, (next8, sum8))
        row2 = lax.broadcasted_iota(jnp.int32, (2, 2 * rows), 0)
        stats[...] = jnp.where(row2 == 0, top, jnp.sum(sum8, axis=0, keepdims=True))
        return next8

    def lanes(h):
        return slice(h * rows, (h + 1) * rows)

    def out_copy(step, d, j, h, to):
        return pltpu.make_async_remote_copy(
            src_ref=osend.at[step, :, lanes(h)],
            dst_ref=oin.at[d, j, :, lanes(h)],
            send_sem=o_ss.at[step, h],
            recv_sem=o_rs.at[d, j, h],
            device_id=to,
            device_id_type=MESH,
        )

    def stat_copy(step, d, j, to):
        return pltpu.make_async_remote_copy(
            src_ref=ssend.at[step],
            dst_ref=sin.at[d, j],
            send_sem=t_ss.at[step],
            recv_sem=t_rs.at[d, j],
            device_id=to,
            device_id_type=MESH,
        )

    def add_arrived(d, j, after):
        with phase("o_wait"):
            stat_copy(0, d, j, sibling).wait_recv()
        top = stats[0:1, :]
        other = sin[d, j, 0:1, :]
        new = jnp.maximum(top, other)
        keep = jnp.exp2(top - new)
        take = jnp.exp2(other - new)
        total = stats[1:2, :] * keep + sin[d, j, 1:2, :] * take
        row2 = lax.broadcasted_iota(jnp.int32, (2, 2 * rows), 0)
        stats[...] = jnp.where(row2 == 0, new, total)
        for h in range(2):
            at = lanes(h)
            with phase("o_wait"):
                out_copy(0, d, j, h, sibling).wait_recv()
            acc[:, at] = acc[:, at] * keep[:, at] + oin[d, j, :, at].astype(F32) * take[:, at]
            after(h)

    def pass_on(step):
        j = half - (step + 1) // 2
        d = 1 - c if step % 2 else c
        to = along_y(lax.rem(y + 1 - 2 * d + ny, ny))

        def send(h):
            if h == 0:
                ssend[step] = stats[...]
                stat_copy(step, d, j - 1, to).start()
            osend[step, :, lanes(h)] = acc[:, lanes(h)].astype(BF16)
            out_copy(step, d, j - 1, h, to).start()

        def plain():
            send(0)
            send(1)

        if j < half - (step % 2):
            add_arrived(d, j, send)
        else:
            plain()

    with phase("first_scores"):
        top8 = first_scores()
    plan = [(0, 1, 0), (1, 0, 0), (1, 1, 1), (1, 1, 0), (1, 0, 0), (1, 1, 1), (1, 0, 0), (1, 1, 1)]
    for step in range(ny):
        with phase("attend"):
            top8 = attend(step, top8)
        if step < ny - 1:
            pass_on(step)
        if step == min(2, ny - 2):
            start_late()
        if step in (5, 7):
            relay_late()
        count_b, count_a, count_wo = plan[step]
        relay_b(count_b)
        relay_a(count_a)
        relay_wo(count_wo)
    def final_stats(d):
        with phase("o_wait"):
            stat_copy(0, d, 0, sibling).wait_recv()

    ways = [None, None]
    top = stats[0:1, :]
    for d in range(2):
        if half > 1:
            final_stats(d)
        else:

            @pl.when(c == d)
            def _():
                final_stats(d)

            @pl.when(c != d)
            def _():
                sin[d, 0] = jnp.full((2, 2 * rows), FLOOR, F32)
                oin[d, 0] = jnp.zeros((HD, 2 * rows), BF16)

        ways[d] = sin[d, 0, 0:1, :]
        top = jnp.maximum(top, ways[d])
    shares = [jnp.exp2(w - top) for w in ways]
    keep = jnp.exp2(stats[0:1, :] - top)
    total = stats[1:2, :] * keep
    for d in range(2):
        total = total + shares[d] * sin[d, 0, 1:2, :]
    keep = keep / total
    shares = [share / total for share in shares]
    got = []
    for h in range(2):
        at = lanes(h)
        for d in range(2):
            with phase("o_wait"):
                wait = out_copy(0, d, 0, h, sibling).wait_recv
                if half > 1:
                    wait()
                else:
                    pl.when(c == d)(wait)
        with phase("join"):
            joined = acc[:, at] * keep[:, at]
            for d in range(2):
                joined = joined + oin[d, 0, :, at].astype(F32) * shares[d][:, at]
            part = joined.T.astype(BF16).reshape(nx, 2, own_rows, HD)
            cols = slice(h * HD, (h + 1) * HD)
            for core in range(2):
                att[core, :, :, cols] = part[:, core]
        for dx in range(nx):
            for dc in range(2):
                if dx + dc:
                    core = 1 - c if dc else c
                    to = (sp, 2 * lax.rem(x + dx, nx) + core)
                    n = 2 * dx + dc - 1
                    copy = remote(
                        att.at[core, :, :, cols],
                        attall.at[tp, :, :, cols],
                        g_ss.at[n, h],
                        g_rs.at[n, h],
                        to,
                    )
                    source = 2 * lax.rem(x - dx + nx, nx) + core
                    got.append((copy, source, dx, dc))
        relay_b(1)
        relay_a(h)
    relay_wo(len(pending_wo))
    core_rows = nx * own_rows
    chunk = min(512, width)

    def project(first, block, source):
        for at in range(0, width, chunk):
            part = dot(block, wo[source, :, at : at + chunk])
            if first:
                low[:, at : at + chunk] = part
            else:
                low[:, at : at + chunk] += part

    with phase("outproj"):
        project(True, att[c].reshape(core_rows, 2 * HD), tp)
    near = sorted(range(len(got) // 2), key=lambda n: (min(got[n][2], nx - got[n][2]), got[n][3]))
    for n, block in enumerate(near):
        copy, source, dx, dc = got[block]
        with phase("ag_wait"):
            copy.wait()
            got[len(near) + block][0].wait()
        if dc:
            with phase("fwo_wait"):
                for at in wo_at[-dx % nx]:
                    wo_forwards[at].wait()
        with phase("outproj"):
            project(False, attall[source].reshape(core_rows, 2 * HD), source)
        if n in (0, 3):
            relay_late()
        if n in (1, 3, 4, 5):
            relay_b(1)
        if n in (1, 3):
            relay_a(1)
    for copy in copies_r:
        copy.wait()
    loads["attn_gain"].wait()
    loads["mlp_gain"].wait()

    def normalize(i, _):
        span = pl.ds(pl.multiple_of(i * own_rows, own_rows), own_rows)
        projected = low[span, :]
        power = jnp.mean(projected * projected, axis=-1, keepdims=True)
        middle = rall[i].astype(F32) + attn_gain[...] * projected * lax.rsqrt(power + 1e-06)
        mid[i] = middle
        middle_power = jnp.mean(middle * middle, axis=-1, keepdims=True)
        nrm[i] = (mlp_gain[...] * middle * lax.rsqrt(middle_power + 1e-06)).astype(BF16)
        return 0

    with phase("norm"):
        lax.fori_loop(0, nx, normalize, 0)
    while pending_b or pending_a:
        relay_b(1)
        relay_a(1)

    def forwarded(w):
        with phase("fwd_wait"):
            for copy in forwards[w]:
                copy.wait()

    normed = nrm[...].reshape(core_rows, width)

    def gate_core(j, _):
        gact[j] = dot(normed, wall[j, 0].reshape(width, hidden))
        return 0

    def up_core(j, _):
        gate = gact[j]
        up = dot(normed, wall[j, 1].reshape(width, hidden))
        hid[j] = (gate / (1.0 + jnp.exp(-gate)) * up).astype(BF16)
        return 0

    zs = max(1, chunk * nz // width)

    size = zs * width // nz
    copies = []

    def down_cols(n):
        sums = 0.0
        for j in range(2):
            w = wall[j, 2, n * zs : (n + 1) * zs].reshape(size, hidden)
            sums += lax.dot_general(
                hid[j], w, (((1,), (1,)), ((), ())), preferred_element_type=F32
            )
        cols = slice(n * size, (n + 1) * size)
        ps2[:, :, cols] = sums.astype(BF16).reshape(nx, own_rows, size)
        for d in range(1, nx):
            to = lax.rem(x + d, nx)
            sems = (s_ss.at[n, d - 1], s_rs.at[n, d - 1])
            copies.append(remote(ps2.at[to, :, cols], pr2.at[x, :, cols], *sems, along_x(to)))

    forwarded(0)
    with phase("ffn_gate"):
        lax.fori_loop(0, 2, gate_core, 0)
    forwarded(1)
    with phase("ffn_up"):
        lax.fori_loop(0, 2, up_core, 0)
    while late_a:
        relay_late()
    forwarded(2)
    with phase("ffn_down"):
        for n in range(nz // zs):
            down_cols(n)

    def summed(send, recv):
        sums = send[x].astype(F32)
        for d in range(1, nx):
            sums = sums + recv[lax.rem(x + d, nx)].astype(F32)
        return sums

    with phase("rs2_wait"):
        for copy in copies:
            copy.wait()
    out[...] = (mid[x] + 0.5 * summed(ps2, pr2)).astype(BF16)
    for ring in (k_ring, q_ring, a1, b1, a2, b2, wo_ring):
        ring.finish()
    for step in range(ny - 1):
        stat_copy(step, 0, 0, sibling).wait_send()
        for h in range(2):
            out_copy(step, 0, 0, h, sibling).wait_send()


def make_local(nz, ny, nx, back):
    def local(
        resid,
        queries,
        keys,
        values,
        log_gates,
        documents,
        out_weight,
        attn_gain,
        mlp_gain,
        gate_weight,
        up_weight,
        down_weight,
    ):
        rows = queries.shape[0]
        own_rows, width = resid.shape
        w_rows, hidden = gate_weight.shape
        dma = pltpu.SemaphoreType.DMA
        x_block = pltpu.VMEM((nx, own_rows, width), BF16)
        kz, ky = nz // 2, ny // 2
        scratch = [
            pltpu.VMEM(queries.shape, BF16),
            pltpu.VMEM(values.shape, BF16),
            pltpu.VMEM(log_gates.shape, F32),
            pltpu.VMEM((1, rows), jnp.int32),
            pltpu.VMEM((1, width), F32),
            pltpu.VMEM((1, width), F32),
            pltpu.VMEM((ny, 2 * HD, 2 * rows), BF16),
            pltpu.VMEM((nz, rows, 2 * HD), BF16),
            pltpu.VMEM((nz, HD + AUG, rows), BF16),
            pltpu.VMEM((ny - 1, HD, 2 * rows), BF16),
            pltpu.VMEM((2, ky, HD, 2 * rows), BF16),
            pltpu.VMEM((ny - 1, 2, 2 * rows), F32),
            pltpu.VMEM((2, ky, 2, 2 * rows), F32),
            pltpu.VMEM((2, 2 * rows), F32),
            pltpu.VMEM((2, back + 1, rows, 2 * rows), F32),
            pltpu.VMEM((HD, 2 * rows), F32),
            pltpu.VMEM((2, nx, own_rows, 2 * HD), BF16),
            pltpu.VMEM((2 * nx, nx, own_rows, 2 * HD), BF16),
            pltpu.VMEM((2 * nx, *out_weight.shape), BF16),
            x_block,
            x_block,
            x_block,
            x_block,
            pltpu.VMEM((nx, own_rows, width), F32),
            pltpu.VMEM((2, 3, nz, ny, w_rows, hidden), BF16),
            pltpu.VMEM((2, nx * own_rows, hidden), F32),
            pltpu.VMEM((2, nx * own_rows, hidden), BF16),
            pltpu.VMEM((nx * own_rows, width), F32),
        ]
        for steps, subs in ((ky, 2), (kz, 2), (kz, 3), (ky, 3), (ky, 3), (kz, 3)):
            scratch += [dma((2, steps, subs)), dma((2, steps, subs))]
        scratch += [dma((3, nz + ny)), dma((3, nz + ny))]
        scratch += [dma((ny - 1, 2)), dma((2, ky, 2)), dma((ny - 1,)), dma((2, ky))]
        scratch += [dma((2, max(nx - 1, 1)))] * 2
        scratch += [dma((2, max(nx // 2, 1), 2))] * 2
        scratch += [dma((2 * nx,))] * 2
        scratch += [dma((2 * nx, 2))] * 2
        scratch += [dma((max(1, width // 512), max(nx - 1, 1)))] * 2
        scratch += [dma((12,))]
        vmem = pl.BlockSpec(memory_space=pltpu.VMEM)
        return pl.pallas_call(
            functools.partial(layer_kernel, nz, ny, nx, back),
            out_shape=jax.ShapeDtypeStruct((own_rows, width), BF16),
            in_specs=[pl.BlockSpec(memory_space=pl.ANY)] * 12,
            out_specs=vmem,
            scratch_shapes=scratch,
            compiler_params=pltpu.CompilerParams(
                collective_id=0, has_side_effects=True, vmem_limit_bytes=60 * 1024 * 1024
            ),
        )(
            resid,
            queries,
            keys,
            values,
            log_gates,
            documents.reshape(1, rows),
            out_weight,
            attn_gain.reshape(1, width),
            mlp_gain.reshape(1, width),
            gate_weight,
            up_weight,
            down_weight.T,
        )

    return local


def solution(mesh, ny=Y_DIM):
    blocks, tp = mesh.shape["sp"], mesh.shape["tp"]
    nz, nx = blocks // ny, tp // 2
    back = min((3 * blocks // 4 + ny - 1) // ny, nz - 1)
    placed = (
        P(("sp", "tp"), None),
        P("sp", "tp"),
        P("sp", "tp"),
        P("sp", "tp"),
        P("tp", None),
        P("sp"),
        P("tp", None),
        P(),
        P(),
        P("sp", "tp"),
        P("sp", "tp"),
        P("tp", "sp"),
    )
    return jax.shard_map(
        make_local(nz, ny, nx, back),
        mesh=mesh,
        in_specs=placed,
        out_specs=P(("sp", "tp"), None),
        check_vma=False,
    )
```

```python
import contextlib
import functools
import math

import jax
import jax.numpy as jnp
from jax import lax
from jax.experimental import pallas as pl
from jax.experimental.pallas import tpu as pltpu
from jax.sharding import PartitionSpec as P

HD = 128
MESH = pl.DeviceIdType.MESH
HIDE = -1e30
FLOOR = -1e20
AUG = 16
F32 = jnp.float32
BF16 = jnp.bfloat16
Y_DIM = 8
A_LANES = (128, 256, 256)
PROFILE = False


def phase(name):
    return jax.named_scope(name) if PROFILE else contextlib.nullcontext()


def dot(a, b):
    return jnp.dot(a, b, preferred_element_type=F32)


class Ring:
    def __init__(self, n, pos, core, device, items, send_sem, recv_sem):
        self.n, self.pos, self.core, self.device, self.items = n, pos, core, device, items
        self.send_sem, self.recv_sem = send_sem, recv_sem
        self.last = n // 2 - 1
        self.copies = {}

    def at(self, step):
        return lax.rem(self.pos + step + 2 * self.n, self.n)

    def send(self, s, subs=None):
        for sub in range(len(self.items)) if subs is None else subs:
            if s < self.last:
                ways = [(0, self.at(-s), self.at(1)), (1, self.at(s), self.at(-1))]
            else:
                way = 1 - 2 * self.core
                ways = [(0, self.at(-way * s), self.at(way))]
            for d, item, to in ways:
                ref = self.items[sub](item)
                copy = pltpu.make_async_remote_copy(
                    src_ref=ref,
                    dst_ref=ref,
                    send_sem=self.send_sem.at[d, s, sub],
                    recv_sem=self.recv_sem.at[d, s, sub],
                    device_id=self.device(to),
                    device_id_type=MESH,
                )
                copy.start()
                self.copies[d, s, sub] = copy

    def wait(self, s, subs=None):
        for sub in range(len(self.items)) if subs is None else subs:
            for d in range(2 if s < self.last else 1):
                self.copies[d, s, sub].wait_recv()

    def arrived(self, s):
        if s < self.last:
            return [self.at(-1 - s), self.at(1 + s)]
        return [self.at(self.n // 2)]

    def finish(self):
        for copy in self.copies.values():
            copy.wait_send()


def layer_kernel(
    nz,
    ny,
    nx,
    back,
    resid,
    q_in,
    k_in,
    v_in,
    gates_in,
    docs_in,
    outw,
    attn_gain_in,
    mlp_gain_in,
    gate_w,
    up_w,
    down_w,
    out,
    q,
    v,
    gates,
    docs,
    attn_gain,
    mlp_gain,
    qa,
    kf,
    vt,
    osend,
    oin,
    ssend,
    sin,
    stats,
    raw,
    acc,
    att,
    attall,
    wo,
    rall,
    nrm,
    ps2,
    pr2,
    mid,
    wall,
    gact,
    hid,
    low,
    q_ss,
    q_rs,
    k_ss,
    k_rs,
    a1_ss,
    a1_rs,
    b1_ss,
    b1_rs,
    a2_ss,
    a2_rs,
    b2_ss,
    b2_rs,
    fwd_ss,
    fwd_rs,
    o_ss,
    o_rs,
    t_ss,
    t_rs,
    x_ss,
    x_rs,
    w_ss,
    w_rs,
    wf_ss,
    wf_rs,
    g_ss,
    g_rs,
    s_ss,
    s_rs,
    l_ss,
):
    sp, tp = lax.axis_index("sp"), lax.axis_index("tp")
    z, y = lax.div(sp, ny), lax.rem(sp, ny)
    x, c = lax.div(tp, 2), lax.rem(tp, 2)
    rows = q.shape[0]
    own_rows, width = resid.shape
    hidden = gate_w.shape[1]
    scale = 1.0 / math.sqrt(HD)
    scale2 = scale * math.log2(math.e)
    la = [min(lanes, hidden - 128) for lanes in A_LANES]

    def along_z(i):
        return (i * ny + y, tp)

    def along_y(i):
        return (z * ny + i, tp)

    def along_x(i):
        return (sp, 2 * i + c)

    sibling = (sp, 2 * x + 1 - c)

    barrier = pltpu.get_barrier_semaphore()
    greet = [along_z(lax.rem(z + d, nz)) for d in ([1, nz - 1] if nz > 2 else [1])]
    greet += [along_y(lax.rem(y + d, ny)) for d in range(1, ny)]
    greet += [along_x(lax.rem(x + d, nx)) for d in range(1, nx)]
    greet += [sibling]
    for device in greet:
        pl.semaphore_signal(barrier, inc=1, device_id=device, device_id_type=MESH)

    loads = {}

    def load(name, src, dst):
        loads[name] = pltpu.make_async_copy(src, dst, l_ss.at[len(loads)])
        loads[name].start()

    load("q", q_in, q)
    load("docs", docs_in, docs)
    load("v", v_in, v)
    load("k", k_in, kf.at[z, :, 0:HD])
    load("gate", gate_w, wall.at[c, 0, z, y])
    load("up", up_w, wall.at[c, 1, z, y])
    load("down", down_w, wall.at[c, 2, z, y])
    load("gates", gates_in, gates)
    load("resid", resid, rall.at[x])
    load("wo", outw, wo.at[tp])
    load("attn_gain", attn_gain_in, attn_gain)
    load("mlp_gain", mlp_gain_in, mlp_gain)

    with phase("prep"):
        loads["docs"].wait()
        loads["q"].wait()
        row16 = lax.broadcasted_iota(jnp.int32, (AUG, rows), 0)
        doc16 = jnp.broadcast_to(docs[...], (AUG, rows))
        for h in range(2):
            qa[y, 0:HD, h * rows : (h + 1) * rows] = (
                q[:, h * HD : (h + 1) * HD].astype(F32).T.astype(BF16)
            )
            one_hot = jnp.where((row16 < 3) & (doc16 == row16), 1.0, 0.0)
            pick = jnp.where((row16 >= 3 + 3 * h) & (row16 < 6 + 3 * h), 1.0, 0.0)
            qa[y, HD : HD + AUG, h * rows : (h + 1) * rows] = (one_hot + pick).astype(BF16)
        loads["v"].wait()
        vt[z, 0:HD, :] = v[...].astype(F32).T.astype(BF16)
        vt[z, HD : HD + AUG, :] = jnp.where(row16 == 0, doc16.astype(F32), 0.0).astype(BF16)
        for name in ("k", "gate", "up", "down"):
            loads[name].wait()

    with phase("barrier_wait"):
        pl.semaphore_wait(barrier, len(greet))

    def remote(src, dst, ss, rs, device):
        copy = pltpu.make_async_remote_copy(
            src_ref=src,
            dst_ref=dst,
            send_sem=ss,
            recv_sem=rs,
            device_id=device,
            device_id_type=MESH,
        )
        copy.start()
        return copy

    k_ring = Ring(
        nz,
        z,
        c,
        along_z,
        [lambda i: kf.at[i, :, 0:HD], lambda i: vt.at[i]],
        k_ss,
        k_rs,
    )
    q_ring = Ring(
        ny,
        y,
        c,
        along_y,
        [
            lambda i: qa.at[i, 0 : HD + AUG, 0:rows],
            lambda i: qa.at[i, 0:HD, rows : 2 * rows],
        ],
        q_ss,
        q_rs,
    )
    a1 = Ring(
        nz,
        z,
        c,
        along_z,
        [lambda i, w=w: wall.at[c, w, i, y, :, 0 : la[w]] for w in range(3)],
        a1_ss,
        a1_rs,
    )
    b1 = Ring(
        ny,
        y,
        c,
        along_y,
        [lambda i, w=w: wall.at[c, w, z, i, :, la[w] : hidden] for w in range(3)],
        b1_ss,
        b1_rs,
    )
    a2 = Ring(
        ny,
        y,
        c,
        along_y,
        [lambda i, w=w: wall.at[c, w, :, i, :, 0 : la[w]] for w in range(3)],
        a2_ss,
        a2_rs,
    )
    b2 = Ring(
        nz,
        z,
        c,
        along_z,
        [lambda i, w=w: wall.at[c, w, i, :, :, la[w] : hidden] for w in range(3)],
        b2_ss,
        b2_rs,
    )
    heads_half = outw.shape[0] // 2
    wo_ring = Ring(
        nx,
        x,
        c,
        along_x,
        [lambda i, u=u: wo.at[2 * i + c, u * heads_half : (u + 1) * heads_half] for u in range(2)],
        w_ss,
        w_rs,
    )

    k_ring.send(0, [0])
    q_ring.send(0, [0])
    a1.send(0)
    b1.send(0)
    k_ring.send(0, [1])
    q_ring.send(0, [1])

    wo_forwards = []
    wo_at = {i: [] for i in range(nx)}

    def forward_wo(i, u, rel):
        piece = wo.at[2 * i + c, u * heads_half : (u + 1) * heads_half]
        at = len(wo_forwards)
        wo_at[rel % nx].append(at)
        wo_forwards.append(remote(piece, piece, wf_ss.at[at], wf_rs.at[at], sibling))

    loads["resid"].wait()
    copies_r = []
    for d in range(1, nx):
        sems = (x_ss.at[1, d - 1], x_rs.at[1, d - 1])
        copies_r.append(remote(rall.at[x], rall.at[x], *sems, along_x(lax.rem(x + d, nx))))
    loads["wo"].wait()
    if nx > 1:
        wo_ring.send(0)
    for u in range(2):
        forward_wo(x, u, 0)
    pending_wo = [(s, u) for s in range(nx // 2) for u in range(2)]

    def relay_wo(count):
        for _ in range(min(count, len(pending_wo))):
            s, u = pending_wo.pop(0)
            with phase("wo_wait"):
                wo_ring.wait(s, [u])
            if s < wo_ring.last:
                wo_ring.send(s + 1, [u])
            rels = (-1 - s, 1 + s) if s < wo_ring.last else (nx // 2,)
            for i, rel in zip(wo_ring.arrived(s), rels):
                forward_wo(i, u, rel)

    def second_head(i):
        seen = qa[i, HD : HD + AUG, 0:rows].astype(F32)
        pick = jnp.where((row16 >= 6) & (row16 < 9), 1.0, 0.0)
        qa[i, HD : HD + AUG, rows : 2 * rows] = jnp.where(row16 < 3, seen, pick).astype(BF16)

    def zero_rows(i, _):
        qa[i, HD + AUG :, :] = jnp.zeros((qa.shape[1] - HD - AUG, 2 * rows), BF16)
        return 0

    lax.fori_loop(0, ny, zero_rows, 0)

    def key_terms(i):
        first = pl.multiple_of(rows * (i * ny + y), rows)
        raised = gates[:, pl.ds(first, rows)] * (-1.0 / scale)
        high = raised.astype(BF16).astype(F32)
        middle = (raised - high).astype(BF16).astype(F32)
        lowest = raised - high - middle
        key_docs = vt[i, HD : HD + AUG, :].astype(F32)[0:1, :]
        terms = jnp.where(row16.astype(F32) == key_docs, 0.0, HIDE)
        terms = jnp.where(row16 < 3, terms, 0.0)
        for h in range(2):
            for j, piece in enumerate((high, middle, lowest)):
                terms = jnp.where(row16 == 3 + 3 * h + j, piece[h : h + 1, :], terms)
        tall = jnp.concatenate([terms, jnp.zeros((HD - AUG, rows), F32)], axis=0)
        kf[i, :, HD : 2 * HD] = tall.T.astype(BF16)

    forwards = [[], [], []]

    def forward(piece, w):
        at = len(forwards[w])
        forwards[w].append(remote(piece, piece, fwd_ss.at[w, at], fwd_rs.at[w, at], sibling))

    def forward_a(i, w):
        forward(wall.at[c, w, :, i, :, 0 : la[w]], w)

    def forward_b(i, w):
        forward(wall.at[c, w, i, :, :, la[w] : hidden], w)

    def step_on(ring, s, subs):
        if s <= ring.last:
            for sub in subs:
                with phase("ring_wait"):
                    ring.wait(s, [sub])
                if s < ring.last:
                    ring.send(s + 1, [sub])

    loads["gates"].wait()
    key_terms(z)
    for s in range(max(nz, ny) // 2):
        step_on(k_ring, s, [0])
        step_on(q_ring, s, [0])
        step_on(a1, s, [0, 1, 2])
        step_on(b1, s, [0, 1, 2])
        if s == b1.last:
            b2.send(0)
        if s == a1.last:
            a2.send(0, [0, 1])
        step_on(k_ring, s, [1])
        step_on(q_ring, s, [1])
        if s <= q_ring.last:
            for i in q_ring.arrived(s):
                second_head(i)
        if s <= k_ring.last:
            for i in k_ring.arrived(s):
                key_terms(i)
    for w in range(3):
        forward_b(z, w)
        if w < 2:
            forward_a(y, w)

    pending_b = [(s, w) for s in range(b2.last + 1) for w in range(3)]
    pending_a = [(s, w) for s in range(a2.last + 1) for w in range(2)]
    late_a = [(s, 2) for s in range(a2.last + 1)]

    def start_late():
        a2.send(0, [2])
        forward_a(y, 2)

    def relay_late():
        relay(a2, late_a, forward_a, 1)

    def relay(ring, pending, onward, count):
        for _ in range(min(count, len(pending))):
            s, w = pending.pop(0)
            with phase("relay_wait"):
                ring.wait(s, [w])
            if s < ring.last:
                ring.send(s + 1, [w])
            for i in ring.arrived(s):
                onward(i, w)

    def relay_a(count):
        relay(a2, pending_a, forward_a, count)

    def relay_b(count):
        relay(b2, pending_b, forward_b, count)

    half = ny // 2
    first_block = jnp.maximum(z - back, 0)
    count = z - first_block

    def query_block(step):
        d = 1 - c if step % 2 else c
        return lax.rem(y + (half - (step + 1) // 2) * (1 - 2 * d) + ny, ny)

    def fold(a, op):
        return op(a.reshape(rows // 8, 8, 2 * rows), axis=0)

    def score(slot, j, i, yq, diagonal):
        found = dot(kf[i], qa[yq])
        if diagonal:
            key_at = lax.broadcasted_iota(jnp.int32, found.shape, 0)
            col = lax.broadcasted_iota(jnp.int32, found.shape, 1)
            query_at = jnp.where(col >= rows, col - rows, col)
            found = jnp.where(query_at - key_at + rows * (yq - y) >= 0, found, HIDE)
        raw[slot, j] = found
        return fold(found, jnp.max)

    def weigh(slot, j, top):
        probs = jnp.exp2(raw[slot, j] * scale2 - top)
        return fold(probs, jnp.sum), probs.astype(BF16)

    def highest(top8):
        return jnp.maximum(jnp.max(top8, axis=0, keepdims=True) * scale2, FLOOR)

    def first_scores():
        yq = query_block(0)
        top8 = score(0, 0, z, yq, True)

        def more(j, top8):
            return jnp.maximum(top8, score(0, j, first_block + j - 1, yq, False))

        return lax.fori_loop(1, count + 1, more, top8)

    def attend(step, top8):
        slot = step % 2
        top = highest(top8)
        ahead = query_block(min(step + 1, ny - 1))
        next8 = score(1 - slot, 0, z, ahead, True)
        sum8, probs = weigh(slot, 0, top)
        acc[...] = dot(vt[z, 0:HD, :], probs)

        def more(j, state):
            next8, sum8 = state
            i = first_block + j - 1
            next8 = jnp.maximum(next8, score(1 - slot, j, i, ahead, False))
            part8, probs = weigh(slot, j, top)
            acc[...] += dot(vt[i, 0:HD, :], probs)
            return next8, sum8 + part8

        next8, sum8 = lax.fori_loop(1, count + 1, more, (next8, sum8))
        row2 = lax.broadcasted_iota(jnp.int32, (2, 2 * rows), 0)
        stats[...] = jnp.where(row2 == 0, top, jnp.sum(sum8, axis=0, keepdims=True))
        return next8

    def lanes(h):
        return slice(h * rows, (h + 1) * rows)

    def out_copy(step, d, j, h, to):
        return pltpu.make_async_remote_copy(
            src_ref=osend.at[step, :, lanes(h)],
            dst_ref=oin.at[d, j, :, lanes(h)],
            send_sem=o_ss.at[step, h],
            recv_sem=o_rs.at[d, j, h],
            device_id=to,
            device_id_type=MESH,
        )

    def stat_copy(step, d, j, to):
        return pltpu.make_async_remote_copy(
            src_ref=ssend.at[step],
            dst_ref=sin.at[d, j],
            send_sem=t_ss.at[step],
            recv_sem=t_rs.at[d, j],
            device_id=to,
            device_id_type=MESH,
        )

    def add_arrived(d, j, after):
        with phase("o_wait"):
            stat_copy(0, d, j, sibling).wait_recv()
        top = stats[0:1, :]
        other = sin[d, j, 0:1, :]
        new = jnp.maximum(top, other)
        keep = jnp.exp2(top - new)
        take = jnp.exp2(other - new)
        total = stats[1:2, :] * keep + sin[d, j, 1:2, :] * take
        row2 = lax.broadcasted_iota(jnp.int32, (2, 2 * rows), 0)
        stats[...] = jnp.where(row2 == 0, new, total)
        for h in range(2):
            at = lanes(h)
            with phase("o_wait"):
                out_copy(0, d, j, h, sibling).wait_recv()
            acc[:, at] = acc[:, at] * keep[:, at] + oin[d, j, :, at].astype(F32) * take[:, at]
            after(h)

    def pass_on(step):
        j = half - (step + 1) // 2
        d = 1 - c if step % 2 else c
        to = along_y(lax.rem(y + 1 - 2 * d + ny, ny))

        def send(h):
            if h == 0:
                ssend[step] = stats[...]
                stat_copy(step, d, j - 1, to).start()
            osend[step, :, lanes(h)] = acc[:, lanes(h)].astype(BF16)
            out_copy(step, d, j - 1, h, to).start()

        def plain():
            send(0)
            send(1)

        if j < half - (step % 2):
            add_arrived(d, j, send)
        else:
            plain()

    with phase("first_scores"):
        top8 = first_scores()
    plan = [(0, 1, 0), (1, 0, 0), (1, 1, 1), (1, 1, 0), (1, 0, 0), (1, 1, 1), (1, 0, 0), (1, 1, 1)]
    for step in range(ny):
        with phase("attend"):
            top8 = attend(step, top8)
        if step < ny - 1:
            pass_on(step)
        if step == min(2, ny - 2):
            start_late()
        if step in (5, 7):
            relay_late()
        count_b, count_a, count_wo = plan[step]
        relay_b(count_b)
        relay_a(count_a)
        relay_wo(count_wo)
    def final_stats(d):
        with phase("o_wait"):
            stat_copy(0, d, 0, sibling).wait_recv()

    ways = [None, None]
    top = stats[0:1, :]
    for d in range(2):
        if half > 1:
            final_stats(d)
        else:

            @pl.when(c == d)
            def _():
                final_stats(d)

            @pl.when(c != d)
            def _():
                sin[d, 0] = jnp.full((2, 2 * rows), FLOOR, F32)
                oin[d, 0] = jnp.zeros((HD, 2 * rows), BF16)

        ways[d] = sin[d, 0, 0:1, :]
        top = jnp.maximum(top, ways[d])
    shares = [jnp.exp2(w - top) for w in ways]
    keep = jnp.exp2(stats[0:1, :] - top)
    total = stats[1:2, :] * keep
    for d in range(2):
        total = total + shares[d] * sin[d, 0, 1:2, :]
    keep = keep / total
    shares = [share / total for share in shares]
    got = []
    for h in range(2):
        at = lanes(h)
        for d in range(2):
            with phase("o_wait"):
                wait = out_copy(0, d, 0, h, sibling).wait_recv
                if half > 1:
                    wait()
                else:
                    pl.when(c == d)(wait)
        with phase("join"):
            joined = acc[:, at] * keep[:, at]
            for d in range(2):
                joined = joined + oin[d, 0, :, at].astype(F32) * shares[d][:, at]
            part = joined.T.astype(BF16).reshape(nx, 2, own_rows, HD)
            cols = slice(h * HD, (h + 1) * HD)
            for core in range(2):
                att[core, :, :, cols] = part[:, core]
        for dx in range(nx):
            for dc in range(2):
                if dx + dc:
                    core = 1 - c if dc else c
                    to = (sp, 2 * lax.rem(x + dx, nx) + core)
                    n = 2 * dx + dc - 1
                    copy = remote(
                        att.at[core, :, :, cols],
                        attall.at[tp, :, :, cols],
                        g_ss.at[n, h],
                        g_rs.at[n, h],
                        to,
                    )
                    source = 2 * lax.rem(x - dx + nx, nx) + core
                    got.append((copy, source, dx, dc))
        relay_b(1)
        relay_a(h)
    relay_wo(len(pending_wo))
    core_rows = nx * own_rows
    chunk = min(512, width)

    def project(first, block, source):
        for at in range(0, width, chunk):
            part = dot(block, wo[source, :, at : at + chunk])
            if first:
                low[:, at : at + chunk] = part
            else:
                low[:, at : at + chunk] += part

    with phase("outproj"):
        project(True, att[c].reshape(core_rows, 2 * HD), tp)
    near = sorted(range(len(got) // 2), key=lambda n: (min(got[n][2], nx - got[n][2]), got[n][3]))
    for n, block in enumerate(near):
        copy, source, dx, dc = got[block]
        with phase("ag_wait"):
            copy.wait()
            got[len(near) + block][0].wait()
        if dc:
            with phase("fwo_wait"):
                for at in wo_at[-dx % nx]:
                    wo_forwards[at].wait()
        with phase("outproj"):
            project(False, attall[source].reshape(core_rows, 2 * HD), source)
        if n in (0, 3):
            relay_late()
        if n in (1, 3, 4, 5):
            relay_b(1)
        if n in (1, 3):
            relay_a(1)
    for copy in copies_r:
        copy.wait()
    loads["attn_gain"].wait()
    loads["mlp_gain"].wait()

    def normalize(i, _):
        span = pl.ds(pl.multiple_of(i * own_rows, own_rows), own_rows)
        projected = low[span, :]
        power = jnp.mean(projected * projected, axis=-1, keepdims=True)
        middle = rall[i].astype(F32) + attn_gain[...] * projected * lax.rsqrt(power + 1e-06)
        mid[i] = middle
        middle_power = jnp.mean(middle * middle, axis=-1, keepdims=True)
        nrm[i] = (mlp_gain[...] * middle * lax.rsqrt(middle_power + 1e-06)).astype(BF16)
        return 0

    with phase("norm"):
        lax.fori_loop(0, nx, normalize, 0)
    while pending_b or pending_a:
        relay_b(1)
        relay_a(1)

    def forwarded(w):
        with phase("fwd_wait"):
            for copy in forwards[w]:
                copy.wait()

    normed = nrm[...].reshape(core_rows, width)

    def gate_core(j, _):
        gact[j] = dot(normed, wall[j, 0].reshape(width, hidden))
        return 0

    def up_core(j, _):
        gate = gact[j]
        up = dot(normed, wall[j, 1].reshape(width, hidden))
        hid[j] = (gate / (1.0 + jnp.exp(-gate)) * up).astype(BF16)
        return 0

    zs = max(1, chunk * nz // width)

    size = zs * width // nz
    copies = []

    def down_cols(n):
        sums = 0.0
        for j in range(2):
            w = wall[j, 2, n * zs : (n + 1) * zs].reshape(size, hidden)
            sums += lax.dot_general(
                hid[j], w, (((1,), (1,)), ((), ())), preferred_element_type=F32
            )
        cols = slice(n * size, (n + 1) * size)
        ps2[:, :, cols] = sums.astype(BF16).reshape(nx, own_rows, size)
        for d in range(1, nx):
            to = lax.rem(x + d, nx)
            sems = (s_ss.at[n, d - 1], s_rs.at[n, d - 1])
            copies.append(remote(ps2.at[to, :, cols], pr2.at[x, :, cols], *sems, along_x(to)))

    forwarded(0)
    with phase("ffn_gate"):
        lax.fori_loop(0, 2, gate_core, 0)
    forwarded(1)
    with phase("ffn_up"):
        lax.fori_loop(0, 2, up_core, 0)
    while late_a:
        relay_late()
    forwarded(2)
    with phase("ffn_down"):
        for n in range(nz // zs):
            down_cols(n)

    for ring in (k_ring, q_ring, a1, b1, a2, b2, wo_ring):
        ring.finish()
    for step in range(ny - 1):
        stat_copy(step, 0, 0, sibling).wait_send()
        for h in range(2):
            out_copy(step, 0, 0, h, sibling).wait_send()
    for n in range(nz // zs):
        with phase("rs2_wait"):
            for copy in copies[n * (nx - 1) : (n + 1) * (nx - 1)]:
                copy.wait()
        cols = slice(n * size, (n + 1) * size)
        sums = ps2[x, :, cols].astype(F32)
        for d in range(1, nx):
            sums = sums + pr2[lax.rem(x + d, nx), :, cols].astype(F32)
        out[:, cols] = (mid[x, :, cols] + 0.5 * sums).astype(BF16)


def make_local(nz, ny, nx, back):
    def local(
        resid,
        queries,
        keys,
        values,
        log_gates,
        documents,
        out_weight,
        attn_gain,
        mlp_gain,
        gate_weight,
        up_weight,
        down_weight,
    ):
        rows = queries.shape[0]
        own_rows, width = resid.shape
        w_rows, hidden = gate_weight.shape
        dma = pltpu.SemaphoreType.DMA
        x_block = pltpu.VMEM((nx, own_rows, width), BF16)
        kz, ky = nz // 2, ny // 2
        scratch = [
            pltpu.VMEM(queries.shape, BF16),
            pltpu.VMEM(values.shape, BF16),
            pltpu.VMEM(log_gates.shape, F32),
            pltpu.VMEM((1, rows), jnp.int32),
            pltpu.VMEM((1, width), F32),
            pltpu.VMEM((1, width), F32),
            pltpu.VMEM((ny, 2 * HD, 2 * rows), BF16),
            pltpu.VMEM((nz, rows, 2 * HD), BF16),
            pltpu.VMEM((nz, HD + AUG, rows), BF16),
            pltpu.VMEM((ny - 1, HD, 2 * rows), BF16),
            pltpu.VMEM((2, ky, HD, 2 * rows), BF16),
            pltpu.VMEM((ny - 1, 2, 2 * rows), F32),
            pltpu.VMEM((2, ky, 2, 2 * rows), F32),
            pltpu.VMEM((2, 2 * rows), F32),
            pltpu.VMEM((2, back + 1, rows, 2 * rows), F32),
            pltpu.VMEM((HD, 2 * rows), F32),
            pltpu.VMEM((2, nx, own_rows, 2 * HD), BF16),
            pltpu.VMEM((2 * nx, nx, own_rows, 2 * HD), BF16),
            pltpu.VMEM((2 * nx, *out_weight.shape), BF16),
            x_block,
            x_block,
            x_block,
            x_block,
            pltpu.VMEM((nx, own_rows, width), F32),
            pltpu.VMEM((2, 3, nz, ny, w_rows, hidden), BF16),
            pltpu.VMEM((2, nx * own_rows, hidden), F32),
            pltpu.VMEM((2, nx * own_rows, hidden), BF16),
            pltpu.VMEM((nx * own_rows, width), F32),
        ]
        for steps, subs in ((ky, 2), (kz, 2), (kz, 3), (ky, 3), (ky, 3), (kz, 3)):
            scratch += [dma((2, steps, subs)), dma((2, steps, subs))]
        scratch += [dma((3, nz + ny)), dma((3, nz + ny))]
        scratch += [dma((ny - 1, 2)), dma((2, ky, 2)), dma((ny - 1,)), dma((2, ky))]
        scratch += [dma((2, max(nx - 1, 1)))] * 2
        scratch += [dma((2, max(nx // 2, 1), 2))] * 2
        scratch += [dma((2 * nx,))] * 2
        scratch += [dma((2 * nx, 2))] * 2
        scratch += [dma((max(1, width // 512), max(nx - 1, 1)))] * 2
        scratch += [dma((12,))]
        vmem = pl.BlockSpec(memory_space=pltpu.VMEM)
        return pl.pallas_call(
            functools.partial(layer_kernel, nz, ny, nx, back),
            out_shape=pltpu.VMEM((own_rows, width), BF16),
            in_specs=[pl.BlockSpec(memory_space=pl.ANY)] * 12,
            out_specs=vmem,
            scratch_shapes=scratch,
            compiler_params=pltpu.CompilerParams(
                collective_id=0, has_side_effects=True, vmem_limit_bytes=60 * 1024 * 1024
            ),
        )(
            resid,
            queries,
            keys,
            values,
            log_gates,
            documents.reshape(1, rows),
            out_weight,
            attn_gain.reshape(1, width),
            mlp_gain.reshape(1, width),
            gate_weight,
            up_weight,
            down_weight.T,
        )

    return local


def solution(mesh, ny=Y_DIM):
    blocks, tp = mesh.shape["sp"], mesh.shape["tp"]
    nz, nx = blocks // ny, tp // 2
    back = min((3 * blocks // 4 + ny - 1) // ny, nz - 1)
    placed = (
        P(("sp", "tp"), None),
        P("sp", "tp"),
        P("sp", "tp"),
        P("sp", "tp"),
        P("tp", None),
        P("sp"),
        P("tp", None),
        P(),
        P(),
        P("sp", "tp"),
        P("sp", "tp"),
        P("tp", "sp"),
    )
    return jax.shard_map(
        make_local(nz, ny, nx, back),
        mesh=mesh,
        in_specs=placed,
        out_specs=P(("sp", "tp"), None),
        check_vma=False,
    )
```
